32 devices in a mesh: sp: 16 (over z, y, x), tp: 2 (over core).
Axes of the slice: x: 2, y: 2, z: 4, core: 2. Of those that a mesh axis runs over, the one named last changes fastest.
Arguments:
- query_logits: bfloat16 [2048, 1024], P('sp', 'tp'), may hold values from -6 to 6
- value_rows: bfloat16 [2048, 1024], P('sp', 'tp'), may hold values from -6 to 6
- onward_forget_logits: bfloat16 [2048, 1024], P('sp', 'tp'), may hold values from -5.5 to 5.5
- reverse_forget_logits: bfloat16 [2048, 1024], P('sp', 'tp'), may hold values from -5.5 to 5.5
- output_gate_logits: bfloat16 [2048, 1024], P('sp', 'tp'), may hold values from -6 to 6
- onward_floor_gap: float32 [1024], P('tp'), may hold values from 0 to 0.12, as said below
- reverse_floor_gap: float32 [1024], P('tp'), may hold values from 0 to 0.12, as said below
- extra_log_decay: float32 [2048, 8], P('sp', 'tp'), may hold values from -2.1 to 0
- per_head_gain: float32 [128], replicated, may hold values from 0.1 to 1.9
- residual: bfloat16 [2048, 2048], P('sp', 'tp'), may hold values from -8 to 8
- output_matrix: bfloat16 [1024, 2048], P(None, 'tp'), may hold values from -0.375 to 0.375
- inner_norm_gain: float32 [2048], P('tp'), may hold values from 0.1 to 1.9
- inner_norm_bias: float32 [2048], P('tp'), may hold values from -1.5 to 1.5
- gate_matrix: bfloat16 [2048, 5632], P('sp', 'tp'), may hold values from -0.125 to 0.125
- up_matrix: bfloat16 [2048, 5632], P('sp', 'tp'), may hold values from -0.125 to 0.125
- down_matrix: bfloat16 [5632, 2048], P('tp', 'sp'), may hold values from -0.15625 to 0.15625
- closing_norm_gain: float32 [2048], P('tp'), may hold values from 0.1 to 1.9
- closing_norm_bias: float32 [2048], P('tp'), may hold values from -1.5 to 1.5
Outputs:
- layer_output: bfloat16 [2048, 2048], P('sp', 'tp')
The draws below stay inside these ranges and needn't reach their ends.
Inputs may be any that keep to these rules, and one draw needn't show every extreme that they name: `onward_floor_gap`: positive. `reverse_floor_gap`: positive.
All inputs are finite; a program needn't handle non-finite values.
Results may differ from the reference program's by a relative error of at most 0.014.
Values may be sent and summed in bfloat16 or wider, within the bound.
A program may use at most 128 MiB of HBM per device.

```python
import math
import jax
import jax.numpy as jnp
from jax import lax

D = 2048
HEADS = 8
HEAD_WIDTH = 128
FF = 5632
TOK_DEV = 128
TOKENS = 2048
N_TP = 2


def forget_values(key):
    block_shift = jax.random.uniform(jax.random.fold_in(key, 11), (TOKENS // TOK_DEV, 1), jnp.float32, -1.5, 1.5)
    shift = jnp.repeat(block_shift, TOK_DEV, axis=0)
    noise = jnp.clip(jax.random.normal(key, (TOKENS, HEADS * HEAD_WIDTH), jnp.float32), -4.0, 4.0)
    return (noise + shift).astype(jnp.bfloat16)


def floor_values(key):
    order = jax.random.permutation(jax.random.fold_in(key, 1), HEADS)
    fast = order < HEADS // 2
    quick = jax.random.uniform(jax.random.fold_in(key, 2), (HEADS, HEAD_WIDTH), jnp.float32, 0.03, 0.12)
    slow = jax.random.uniform(jax.random.fold_in(key, 3), (HEADS, HEAD_WIDTH), jnp.float32, 0.3, 1.2) / TOKENS
    return jnp.where(fast[:, None], quick, slow).reshape(HEADS * HEAD_WIDTH).astype(jnp.float32)


def draw_onward_forget_logits(key, part):
    return forget_values(jax.random.fold_in(key, 101))


def draw_reverse_forget_logits(key, part):
    return forget_values(jax.random.fold_in(key, 202))


def draw_onward_floor_gap(key, part):
    return floor_values(jax.random.fold_in(key, 303))


def draw_reverse_floor_gap(key, part):
    return floor_values(jax.random.fold_in(key, 404))


def draw_extra_log_decay(key, part):
    inner = jax.random.fold_in(key, 505)
    spots = jax.random.randint(jax.random.fold_in(inner, 1), (3, HEADS), 0, TOKENS)
    depth = jnp.log(jax.random.uniform(jax.random.fold_in(inner, 2), (3, HEADS), jnp.float32, 0.5, 0.8))
    places = jnp.arange(TOKENS, dtype=jnp.int32)[:, None, None] == spots[None]
    return jnp.sum(jnp.where(places, depth[None], 0.0), axis=1).astype(jnp.float32)


def draw_residual(key, part):
    inner = jax.random.fold_in(key, 606)
    ramp = 0.6 + 1.2 * jnp.arange(D, dtype=jnp.float32) / D
    base = jax.random.normal(inner, (TOKENS, D), jnp.float32)
    return jnp.clip(base * ramp, -8.0, 8.0).astype(jnp.bfloat16)


def shard_levels(stream_key, extent, pieces, smallest, largest):
    def one(dim, shards_of):
        steps = jax.random.uniform(jax.random.fold_in(jax.random.fold_in(stream_key, 6), dim), (shards_of,), jnp.float32, smallest / len(pieces), largest / len(pieces))
        return jnp.repeat(jnp.exp(steps), extent[dim] // shards_of).reshape((-1,) + (1,) * (len(extent) - dim - 1))

    level = one(*pieces[0])
    for cut in pieces[1:]:
        level = level * one(*cut)
    return level


def bell_draw(key, shape, scale, limit, cuts=(), kind=jnp.bfloat16):
    level = shard_levels(key, shape, cuts, -0.22, 0.18) if cuts else 1.0
    values = jax.random.normal(key, shape, jnp.float32) * scale * level
    return jnp.minimum(jnp.maximum(values, -limit), limit).astype(kind)


def setup_inputs(seed: int = 0) -> dict:
    arg_keys = jax.random.split(jax.random.key(seed), 19)
    return {
        "query_logits": bell_draw(arg_keys[0], (TOKENS, HEADS * HEAD_WIDTH), 1.0, 6.0, ((0, 16), (1, 2))),
        "value_rows": bell_draw(arg_keys[1], (TOKENS, HEADS * HEAD_WIDTH), 1.0, 6.0, ((0, 16), (1, 2))),
        "onward_forget_logits": draw_onward_forget_logits(jax.random.fold_in(arg_keys[18], 71), 0),
        "reverse_forget_logits": draw_reverse_forget_logits(jax.random.fold_in(arg_keys[18], 71), 0),
        "output_gate_logits": bell_draw(arg_keys[4], (TOKENS, HEADS * HEAD_WIDTH), 1.0, 6.0, ((0, 16), (1, 2))),
        "onward_floor_gap": draw_onward_floor_gap(jax.random.fold_in(arg_keys[18], 71), 0),
        "reverse_floor_gap": draw_reverse_floor_gap(jax.random.fold_in(arg_keys[18], 71), 0),
        "extra_log_decay": draw_extra_log_decay(jax.random.fold_in(arg_keys[18], 71), 0),
        "per_head_gain": jnp.clip(1.0 + 0.18 * jax.random.normal(arg_keys[8], (HEAD_WIDTH,), jnp.float32), 0.1, 1.9),
        "residual": draw_residual(jax.random.fold_in(arg_keys[18], 71), 0),
        "output_matrix": bell_draw(arg_keys[10], (HEADS * HEAD_WIDTH, D), (HEADS * HEAD_WIDTH // 4) ** -0.5, 0.375, ((1, 2),)),
        "inner_norm_gain": jnp.clip(1.0 + 0.18 * jax.random.normal(arg_keys[11], (D,), jnp.float32), 0.1, 1.9),
        "inner_norm_bias": bell_draw(arg_keys[12], (D,), 0.3, 1.5, ((0, 2),), jnp.float32),
        "gate_matrix": bell_draw(arg_keys[13], (D, FF), D ** -0.5, 0.125, ((0, 16), (1, 2))),
        "up_matrix": bell_draw(arg_keys[14], (D, FF), D ** -0.5, 0.125, ((0, 16), (1, 2))),
        "down_matrix": bell_draw(arg_keys[15], (FF, D), (FF // 4) ** -0.5, 0.15625, ((0, 2), (1, 16))),
        "closing_norm_gain": jnp.clip(1.0 + 0.18 * jax.random.normal(arg_keys[16], (D,), jnp.float32), 0.1, 1.9),
        "closing_norm_bias": bell_draw(arg_keys[17], (D,), 0.3, 1.5, ((0, 2),), jnp.float32),
    }


highest_precision = lax.Precision.HIGHEST
alpha_mix = 2.0 ** 0.25
norm_eps = 1e-05
head_eps = 1e-06

def decay_factors(unscaled_input, lower_bound_gap, extra_decays):
    decay_factor = lower_bound_gap * jax.nn.sigmoid(-unscaled_input.astype(jnp.float32))
    return (jnp.log1p(-decay_factor) + extra_decays, decay_factor)

def recurrence(query, keys, values, log_decay):
    total, head_count, model_width = query.shape
    span = math.gcd(total, 128)
    count = total // span
    triangle = jnp.tril(jnp.ones((span, span), jnp.float32))

    def blocks(array):
        return array.reshape(count, span, head_count, array.shape[2])

    def advance(running_state, inputs):
        query_block, key_block, value_tile, log_block = inputs
        running = jnp.cumsum(log_block, axis=0)
        final_index = running[-1]
        decayed_query = query_block * jnp.exp(running)
        key_inverse = key_block * jnp.exp(-running)
        key_stop = key_block * jnp.exp(final_index[None] - running)
        scores = jnp.einsum('thk,shk->hts', decayed_query, key_inverse, precision=highest_precision) * triangle[None]
        inner = jnp.einsum('hts,shv->thv', scores, value_tile, precision=highest_precision)
        carried_state = jnp.einsum('nex,exl->nel', decayed_query, running_state, precision=highest_precision)
        running_state = jnp.exp(final_index)[:, :, None] * running_state + jnp.einsum('ojy,oje->jye', key_stop, value_tile, precision=highest_precision)
        return (running_state, inner + carried_state)
    start = jnp.zeros((head_count, model_width, values.shape[2]), jnp.float32)
    final, outputs = lax.scan(advance, start, (blocks(query), blocks(keys), blocks(values), blocks(log_decay)))
    return outputs.reshape(total, head_count, values.shape[2])

def layer_norm(rows, gain, bias):
    centre = rows - lax.optimization_barrier(jnp.mean(rows, axis=-1, keepdims=True))
    spread = lax.optimization_barrier(jnp.mean(centre * centre, axis=-1, keepdims=True))
    return centre * lax.rsqrt(spread + norm_eps) * gain + bias

def reference(query_logits, value_rows, onward_forget_logits, reverse_forget_logits, output_gate_logits, onward_floor_gap, reverse_floor_gap, extra_log_decay, per_head_gain, residual, output_matrix, inner_norm_gain, inner_norm_bias, gate_matrix, up_matrix, down_matrix, closing_norm_gain, closing_norm_bias):
    total = query_logits.shape[0]
    shape_head = (total, HEADS, HEAD_WIDTH)
    query = jax.nn.silu(query_logits.astype(jnp.float32)).reshape(shape_head)
    values = value_rows.astype(jnp.float32).reshape(shape_head)
    extra_decays = jnp.repeat(extra_log_decay, HEAD_WIDTH, axis=1)
    onward_log_decay, onward_key_rows = decay_factors(onward_forget_logits, onward_floor_gap, extra_decays)
    reverse_log_decay, reverse_key_rows = decay_factors(reverse_forget_logits, reverse_floor_gap, extra_decays)
    upcoming_part = recurrence(query, onward_key_rows.reshape(shape_head), values, onward_log_decay.reshape(shape_head))
    preceding_part = jnp.flip(recurrence(jnp.flip(query, axis=0), jnp.flip(reverse_key_rows.reshape(shape_head), axis=0), jnp.flip(values, axis=0), jnp.flip(reverse_log_decay.reshape(shape_head), axis=0)), axis=0)
    mixed = upcoming_part + preceding_part
    normed = mixed * lax.rsqrt(lax.optimization_barrier(jnp.mean(mixed * mixed, axis=2, keepdims=True)) + head_eps) * per_head_gain
    gated = (normed.reshape(total, HEADS * HEAD_WIDTH) * jax.nn.silu(output_gate_logits.astype(jnp.float32))).astype(jnp.bfloat16)
    piece_rows = math.gcd(total, 2048)
    count = total // piece_rows
    share = FF // N_TP

    def finish(inputs):
        gated_rows, residual_rows = inputs
        mixer = jnp.dot(gated_rows, output_matrix, preferred_element_type=jnp.float32)
        middle = layer_norm(alpha_mix * residual_rows.astype(jnp.float32) + mixer, inner_norm_gain, inner_norm_bias).astype(jnp.bfloat16)
        gate = jnp.dot(middle, gate_matrix, preferred_element_type=jnp.float32)
        up = jnp.dot(middle, up_matrix, preferred_element_type=jnp.float32)
        hidden = (jax.nn.silu(gate) * up).astype(jnp.bfloat16)
        feed = jnp.zeros((piece_rows, D), jnp.float32)
        for part_index in range(N_TP):
            term = jnp.dot(hidden[:, part_index * share:(part_index + 1) * share], down_matrix[part_index * share:(part_index + 1) * share], preferred_element_type=jnp.float32).astype(jnp.bfloat16)
            feed = feed + lax.optimization_barrier(term).astype(jnp.float32)
        return layer_norm(alpha_mix * middle.astype(jnp.float32) + feed, closing_norm_gain, closing_norm_bias).astype(jnp.bfloat16)
    result = lax.map(finish, (gated.reshape(count, piece_rows, HEADS * HEAD_WIDTH), residual.reshape(count, piece_rows, D)))
    return result.reshape(total, D)
```

```python
import functools
import math

import jax
import jax.numpy as jnp
from jax import lax
from jax.experimental import pallas as pl
from jax.experimental.pallas import tpu as pltpu
from jax.sharding import PartitionSpec as P

highest = lax.Precision.HIGHEST
alpha_mix = 2.0**0.25
norm_eps = 1e-05
head_eps = 1e-06
bf16 = jnp.bfloat16
f32 = jnp.float32
MESH = pl.DeviceIdType.MESH


def pick(table, at):
    out = jnp.int32(table[0])
    for i, value in enumerate(table[1:], 1):
        out = jnp.where(at == i, jnp.int32(value), out)
    return out


def across(x, w):
    return lax.dot_general(x, w, (((1,), (1,)), ((), ())), preferred_element_type=f32)


def silu(x):
    return x / (1.0 + jnp.exp(-x))


def layer_kernel(
    far, near, cores,
    q_ref, v_ref, f_ref, r_ref, og_ref, fg_ref, rg_ref, ex_ref, hg_ref, res_ref, om_ref, ig_ref,
    ib_ref, gate_ref, up_ref, down_ref, cg_ref, cb_ref, out_ref,
    wbuf, dbuf, wsend, st_send, tot_send, st_recv, tot_recv, fs_send, ft_send, f_recv, ft_recv,
    b_send, b_recv, om_all, res_all, ig_all, ib_all, g_all, x_all, inner, dq, hid, ts_send,
    ts_recv, rs_send, rs_recv, fin_all, xs,
    deal_s, deal_r, ring_s, ring_r, s1_s, s1_r, s2_s, s2_r, s3_s, s3_r, tp_s, tp_r, ga_s, ga_r,
    ag_s, ag_r, d2_s, d2_r, ts_s, ts_r, rs_s, rs_r, fin_s, fin_r, own_s,
):
    rows = q_ref.shape[0]
    heads, width = ex_ref.shape[1], hg_ref.shape[1]
    units, deep = dbuf.shape[2:]
    chunk = st_send.shape[2]
    per_head = near // heads
    share = near // cores
    half = (units // 2 + 15) // 16 * 16
    n2 = near // 2
    me, core = lax.axis_index("sp"), lax.axis_index("tp")
    z, p = me // near, me % near

    ring = [i ^ (i >> 1) for i in range(near)]
    spot = [ring.index(i) for i in range(near)]
    right = pick([ring[(spot[i] + 1) % near] for i in range(near)], p)
    left = pick([ring[(spot[i] - 1) % near] for i in range(near)], p)

    def behind(sign, d):
        return pick([ring[(spot[i] - sign * d) % near] for i in range(near)], p)

    partners = [sorted((j for j in range(far) if j != i), key=lambda j: (abs(j - i), j))
                for i in range(far)]
    order = [z] + [pick([partners[i][k] for i in range(far)], z) for k in range(far - 1)]

    sends = []

    def copy(src, dst, ssem, rsem, to):
        return pltpu.make_async_remote_copy(
            src_ref=src, dst_ref=dst, send_sem=ssem, recv_sem=rsem, device_id=to,
            device_id_type=MESH,
        )

    def start(c, when=None):
        sends.append((c, when))
        if when is None:
            c.start()
        else:
            pl.when(when)(c.start)

    def landed(c, when=None):
        if when is None:
            c.wait_recv()
        else:
            pl.when(when)(c.wait_recv)

    def at(zz, pp):
        return (zz * near + pp, core)

    def mate(m):
        return (me, (core + m) % cores)

    f_recv[...] = jnp.zeros_like(f_recv)
    ft_recv[...] = jnp.zeros_like(ft_recv)

    barrier = pltpu.get_barrier_semaphore()
    peers = [at(z, (p + j) % near) for j in range(1, near)]
    peers += [at((z + j) % far, p) for j in range(1, far)]
    peers += [mate(m) for m in range(1, cores)]
    for peer in peers:
        pl.semaphore_signal(barrier, inc=1, device_id=peer, device_id_type=MESH)

    own_om = pltpu.make_async_copy(om_ref, om_all.at[core], own_s.at[0])
    own_om.start()
    for i, ref in enumerate((gate_ref, up_ref)):
        whole = ref[...].astype(f32).T
        for j in range(far):
            wsend[j, i] = whole[j * units : (j + 1) * units].astype(bf16)
    wbuf[p, z] = wsend[z]
    dbuf[p, z] = down_ref[pl.ds(pl.multiple_of(z * units, 16), units), :]
    res_all[core] = res_ref[...]
    ig_all[core] = ig_ref[...]
    ib_all[core] = ib_ref[...]
    pl.semaphore_wait(barrier, len(peers))

    def deal_copy(g, k, out):
        zz = order[k + 1]
        if g == 0:
            src, dst = wsend.at[zz], wbuf
        else:
            src, dst = down_ref.at[pl.ds(pl.multiple_of(zz * units, 16), units), :], dbuf
        slot = z if out else zz
        return copy(src, dst.at[p, slot], deal_s.at[g, k], deal_r.at[g, slot], at(zz, p))

    def deal(g, k):
        start(deal_copy(g, k, True))

    def ring_copy(k, sign, d, block):
        g, zz = k // far, order[k % far]
        buf = dbuf if g else wbuf
        side = 0 if sign > 0 else 1
        ref = buf.at[block, zz]
        if d == n2:
            if g:
                ref = ref.at[pl.ds(0, half), :] if side == 0 else ref.at[pl.ds(half, units - half), :]
            else:
                ref = ref.at[pl.ds(side, 1)]
        to = right if sign > 0 else left
        return copy(ref, ref, ring_s.at[side, d - 1, k], ring_r.at[side, d - 1, k], at(z, to))

    def ring_start(k):
        if k % far:
            landed(deal_copy(k // far, k % far - 1, False))
        for sign in (1, -1):
            start(ring_copy(k, sign, 1, p))

    def ring_forward(k):
        for d in range(1, n2):
            for sign in (1, -1):
                block = behind(sign, d)
                landed(ring_copy(k, sign, d, block))
                start(ring_copy(k, sign, d + 1, block))

    def ring_done(k):
        for sign in (1, -1):
            landed(ring_copy(k, sign, n2, behind(sign, n2)))

    for k in range(far - 1):
        deal(0, k)
    ring_start(0)

    pairs = ((om_ref, om_all), (res_ref, res_all), (ig_ref, ig_all), (ib_ref, ib_all))

    def tp_copy(i, m, out):
        src, dst = pairs[i]
        slot = core if out else (core + cores - m) % cores
        return copy(src, dst.at[slot], tp_s.at[i, m], tp_r.at[i, m], mate(m))

    for m in range(1, cores):
        for i in range(len(pairs)):
            start(tp_copy(i, m, True))

    t = lax.broadcasted_iota(jnp.int32, (rows, rows), 0)
    s = lax.broadcasted_iota(jnp.int32, (rows, rows), 1)
    lower, upper = s <= t, s >= t
    for h in range(heads):
        cols = slice(h * width, (h + 1) * width)
        q = silu(q_ref[:, cols].astype(f32))
        v = v_ref[:, cols]
        extra = ex_ref[:, h : h + 1]
        scores = jnp.zeros((rows, rows), f32)
        for d, (raw_ref, gap_ref, tri) in enumerate(
            ((f_ref, fg_ref, lower), (r_ref, rg_ref, upper))
        ):
            raw = raw_ref[:, cols].astype(f32)
            key = gap_ref[:, cols] * (1.0 / (1.0 + jnp.exp(raw)))
            log = jnp.log1p(-key) + extra
            run = jnp.dot(tri.astype(f32), log, precision=highest, preferred_element_type=f32)
            last = run[rows - 1 :, :] if d == 0 else run[:1, :]
            qd = (q * jnp.exp(run)).astype(bf16)
            ki = (key * jnp.exp(-run)).astype(bf16)
            ks = (key * jnp.exp(last - run)).astype(bf16)
            scores = scores + jnp.where(tri, across(qd, ki), 0.0)
            dq[d, :, cols] = qd
            state = lax.dot_general(v, ks, (((0,), (0,)), ((), ())), preferred_element_type=f32)
            for i in range(per_head):
                st_send[h * per_head + i, d] = state[i * chunk : (i + 1) * chunk].astype(bf16)
                tot_send[h * per_head + i, d] = last
        inner[:, cols] = jnp.dot(scores.astype(bf16), v, preferred_element_type=f32)

    def plane_copy(i, j, out):
        src, dst = ((st_send, st_recv), (tot_send, tot_recv))[i]
        to = (p + j) % near
        slot = p if out else (p + near - j) % near
        return copy(src.at[to], dst.at[slot], s1_s.at[i, j], s1_r.at[i, j], at(z, to))

    for j in range(1, near):
        for i in range(2):
            start(plane_copy(i, j, True))
    st_recv[p] = st_send[p]
    tot_recv[p] = tot_send[p]

    ring_forward(0)

    for j in range(1, near):
        for i in range(2):
            landed(plane_copy(i, j, False))

    prefix = [[None] * near, [None] * near]
    gone = [[None] * near, [None] * near]
    for d in range(2):
        state = jnp.zeros((chunk, width), f32)
        total = jnp.zeros((1, width), f32)
        for b in range(near) if d == 0 else reversed(range(near)):
            prefix[d][b], gone[d][b] = state, total
            step = tot_recv[b, d]
            state = state * jnp.exp(step) + st_recv[b, d].astype(f32)
            total = total + step
        fs_send[d] = state.astype(bf16)
        ft_send[d] = total

    def far_copy(i, d, e):
        src, dst = ((fs_send, f_recv), (ft_send, ft_recv))[i]
        to = (z + e) % far if d == 0 else (z + far - e) % far
        return copy(src.at[d], dst.at[d, e], s2_s.at[i, d, e], s2_r.at[i, d, e], at(to, p))

    def far_valid(d, e, out):
        return z + e < far if (d == 0) == out else z >= e

    for e in range(1, far):
        for d in range(2):
            for i in range(2):
                start(far_copy(i, d, e), far_valid(d, e, True))

    ring_start(1)

    for e in range(1, far):
        for d in range(2):
            for i in range(2):
                landed(far_copy(i, d, e), far_valid(d, e, False))

    for d in range(2):
        enter = jnp.zeros((chunk, width), f32)
        for e in reversed(range(1, far)):
            enter = enter * jnp.exp(ft_recv[d, e]) + f_recv[d, e].astype(f32)
        for b in range(near):
            b_send[b, d] = (enter * jnp.exp(gone[d][b]) + prefix[d][b]).astype(bf16)

    def back_copy(j, out):
        to = (p + j) % near
        slot = p if out else (p + near - j) % near
        return copy(b_send.at[to], b_recv.at[slot], s3_s.at[j], s3_r.at[j], at(z, to))

    for j in range(1, near):
        start(back_copy(j, True))
    b_recv[p] = b_send[p]

    ring_start(far)

    for j in range(1, near):
        landed(back_copy(j, False))

    for h in range(heads):
        cols = slice(h * width, (h + 1) * width)
        mixed = inner[:, cols]
        for d in range(2):
            state = jnp.concatenate(
                [b_recv[h * per_head + i, d].astype(f32) for i in range(per_head)], axis=0
            ).astype(bf16)
            mixed = mixed + across(dq[d, :, cols], state)
        normed = (
            mixed
            * lax.rsqrt(jnp.mean(mixed * mixed, axis=1, keepdims=True) + head_eps)
            * hg_ref[...]
        )
        g_all[core, :, cols] = (normed * silu(og_ref[:, cols].astype(f32))).astype(bf16)

    def gated_copy(m, out):
        slot = core if out else (core + cores - m) % cores
        return copy(g_all.at[slot], g_all.at[slot], ga_s.at[m], ga_r.at[m], mate(m))

    for m in range(1, cores):
        start(gated_copy(m, True))
    own_om.wait()
    for m in range(1, cores):
        for i in range(len(pairs)):
            landed(tp_copy(i, m, False))
    for m in range(1, cores):
        landed(gated_copy(m, False))

    span = q_ref.shape[1]
    parts = []
    for b in range(cores):
        mixer = alpha_mix * res_all[b].astype(f32)
        for m in range(cores):
            mixer = mixer + jnp.dot(
                g_all[m], om_all[b, m * span : (m + 1) * span, :], preferred_element_type=f32
            )
        parts.append(mixer)
    wide = parts[0].shape[1]
    model = cores * wide
    mean = sum(jnp.sum(x, axis=1, keepdims=True) for x in parts) / model
    parts = [x - mean for x in parts]
    var = sum(jnp.sum(x * x, axis=1, keepdims=True) for x in parts) / model
    scale = lax.rsqrt(var + norm_eps)
    for b, x in enumerate(parts):
        x_all[z, b] = (x * scale * ig_all[b] + ib_all[b]).astype(bf16)

    def line_copy(sign, d):
        block = (z + far + (1 - d) * sign) % far
        side = 0 if sign > 0 else 1
        ref = x_all.at[block, core]
        return copy(ref, ref, ag_s.at[side, d], ag_r.at[side, d], at((z + far + sign) % far, p))

    def line_land(sign, d):
        block = (z + far - d * sign) % far
        side = 0 if sign > 0 else 1
        ref = x_all.at[block, core]
        return copy(ref, ref, ag_s.at[side, d], ag_r.at[side, d], at((z + far + sign) % far, p))

    def line_out(sign, d):
        return jnp.logical_and(z + 1 < far, z >= d - 1) if sign > 0 else jnp.logical_and(z > 0, z + d - 1 < far)

    def line_in(sign, d):
        return z >= d if sign > 0 else z + d < far

    def line_share(sign, d, m, out):
        block = (z + far - d * sign) % far
        side = 0 if sign > 0 else 1
        slot = core if out else (core + cores - m) % cores
        ref = x_all.at[block, slot]
        return copy(ref, ref, d2_s.at[side, d, m], d2_r.at[side, d, m], mate(m))

    def line_step(d):
        for sign in (1, -1):
            landed(line_land(sign, d), line_in(sign, d))
            if d + 1 < far:
                start(line_copy(sign, d + 1), line_out(sign, d + 1))
            for m in range(1, cores):
                start(line_share(sign, d, m, True), line_in(sign, d))

    for sign in (1, -1):
        start(line_copy(sign, 1), line_out(sign, 1))
    ring_forward(1)
    ring_start(2)
    ring_forward(far)
    line_step(1)
    ring_forward(2)
    line_step(2)
    ring_start(3)
    deal(1, 0)
    for d in range(3, far):
        line_step(d)
    for k in range(1, far - 1):
        deal(1, k)
    ring_forward(3)
    for k in range(4, far):
        ring_start(k)
        ring_forward(k)
    for d in range(1, far):
        for sign in (1, -1):
            for m in range(1, cores):
                landed(line_share(sign, d, m, False), line_in(sign, d))
    ring_start(far + 1)
    for k in range(far):
        ring_done(k)

    step = 256
    for n0 in range(0, units, step):
        n1 = min(units, n0 + step)
        gate = up = 0.0
        for pp in range(near):
            spots = [(zz * near + pp) * deep for zz in range(far)]
            x = jnp.concatenate(
                [
                    jnp.concatenate(
                        [x_all[j, c // wide, :, c % wide : c % wide + deep] for c in spots], axis=1
                    )
                    for j in range(far)
                ],
                axis=0,
            )
            wg, wu = (
                jnp.concatenate([wbuf[pp, zz, i, n0:n1, :] for zz in range(far)], axis=1)
                for i in range(2)
            )
            gate = gate + across(x, wg)
            up = up + across(x, wu)
        hid[:, n0:n1] = (silu(gate) * up).astype(bf16)

    def sum_copy(k, m):
        return copy(
            ts_send.at[k, (core + m) % cores], ts_recv.at[k, m], ts_s.at[k, m], ts_r.at[k, m],
            mate(m),
        )

    def reduce_copy(k, j, out):
        zz, to = order[k], order[j + 1]
        src, dst = rs_send.at[k, to], rs_recv.at[z, zz]
        return copy(src, dst, rs_s.at[k, j], rs_r.at[zz, z], at(to, p))

    def down(k):
        zz = order[k]
        w = jnp.concatenate([dbuf[pp, zz] for pp in range(near)], axis=1)
        y = jnp.dot(hid[...], w, preferred_element_type=f32).astype(bf16)
        for c in range(cores):
            ts_send[k, c] = y[:, c * share * deep : (c + 1) * share * deep]
        for m in range(1, cores):
            start(sum_copy(k, m))

    def reduce(k):
        total = ts_send[k, core].astype(f32)
        for m in range(1, cores):
            landed(sum_copy(k, m))
            total = total + ts_recv[k, m].astype(f32)
        total = total.astype(bf16)
        for j in range(far):
            rs_send[k, j] = total[j * rows : (j + 1) * rows]
        for j in reversed(range(far - 1)):
            start(reduce_copy(k, j, True))
        rs_recv[z, order[k]] = rs_send[k, z]

    ring_done(far)
    down(0)
    ring_forward(far + 1)
    if far > 2:
        ring_start(far + 2)
    reduce(0)
    for k in range(1, far):
        ring_done(far + k)
        down(k)
        if k + 1 < far:
            ring_forward(far + k + 1)
        if k + 2 < far:
            ring_start(far + k + 2)
        reduce(k)

    mine = []
    for zz in range(far):
        total = None
        for src in range(far):
            landed(
                copy(rs_send.at[0, 0], rs_recv.at[src, zz], rs_s.at[0, 0], rs_r.at[zz, src], at(src, p)),
                z != src,
            )
            one = rs_recv[src, zz].astype(f32)
            total = one if total is None else total + one
        mine.append(total)
    fin_all[core] = jnp.concatenate(mine, axis=1).astype(bf16)

    def final_copy(m, out):
        slot = core if out else (core + cores - m) % cores
        return copy(fin_all.at[slot], fin_all.at[slot], fin_s.at[m], fin_r.at[m], mate(m))

    for m in range(1, cores):
        start(final_copy(m, True))
    for m in range(1, cores):
        landed(final_copy(m, False))
    feed = [fin_all[c].astype(f32) for c in range(cores)]
    whole = jnp.concatenate(
        [
            feed[pp // share][:, (zz * share + pp % share) * deep : (zz * share + pp % share + 1) * deep]
            for zz in range(far)
            for pp in range(near)
        ],
        axis=1,
    )
    parts = [
        alpha_mix * x_all[z, b].astype(f32) + whole[:, b * wide : (b + 1) * wide]
        for b in range(cores)
    ]
    mean = sum(jnp.sum(x, axis=1, keepdims=True) for x in parts) / model
    parts = [x - mean for x in parts]
    var = sum(jnp.sum(x * x, axis=1, keepdims=True) for x in parts) / model
    scale = lax.rsqrt(var + norm_eps)
    for b, x in enumerate(parts):
        xs[b] = x * scale
    out_ref[...] = (xs[core] * cg_ref[...] + cb_ref[...]).astype(bf16)

    for c, when in sends:
        if when is None:
            c.wait_send()
        else:
            pl.when(when)(c.wait_send)


def shards(
    query_logits, value_rows, onward_forget_logits, reverse_forget_logits, output_gate_logits,
    onward_floor_gap, reverse_floor_gap, extra_log_decay, per_head_gain, residual, output_matrix,
    inner_norm_gain, inner_norm_bias, gate_matrix, up_matrix, down_matrix,
    closing_norm_gain, closing_norm_bias,
):
    count, cores = lax.axis_size("sp"), lax.axis_size("tp")
    far = math.gcd(count, 4)
    near = count // far
    rows, span = query_logits.shape
    heads = extra_log_decay.shape[1]
    width = span // heads
    wide = residual.shape[1]
    units = gate_matrix.shape[1] // far
    deep = gate_matrix.shape[0]
    chunk = heads * width // near
    share = near // cores
    n2 = near // 2
    inner_rows = output_matrix.shape[0]
    vm = pltpu.VMEM
    dma = lambda *shape: pltpu.SemaphoreType.DMA(shape)
    scratch = [
        vm((near, far, 2, units, deep), bf16), vm((near, far, units, deep), bf16),
        vm((far, 2, units, deep), bf16),
        vm((near, 2, chunk, width), bf16), vm((near, 2, 1, width), f32),
        vm((near, 2, chunk, width), bf16), vm((near, 2, 1, width), f32),
        vm((2, chunk, width), bf16), vm((2, 1, width), f32),
        vm((2, far, chunk, width), bf16), vm((2, far, 1, width), f32),
        vm((near, 2, chunk, width), bf16), vm((near, 2, chunk, width), bf16),
        vm((cores, inner_rows, wide), bf16), vm((cores, rows, wide), bf16),
        vm((cores, 1, wide), f32), vm((cores, 1, wide), f32),
        vm((cores, rows, span), bf16), vm((far, cores, rows, wide), bf16),
        vm((rows, span), f32), vm((2, rows, span), bf16), vm((far * rows, units), bf16),
        vm((far, cores, far * rows, share * deep), bf16),
        vm((far, cores, far * rows, share * deep), bf16),
        vm((far, far, rows, share * deep), bf16), vm((far, far, rows, share * deep), bf16),
        vm((cores, rows, far * share * deep), bf16), vm((cores, rows, wide), f32),
        dma(2, far), dma(2, far), dma(2, n2, 2 * far), dma(2, n2, 2 * far),
        dma(2, near), dma(2, near), dma(2, 2, far), dma(2, 2, far), dma(near), dma(near),
        dma(4, cores), dma(4, cores), dma(cores), dma(cores), dma(2, far), dma(2, far),
        dma(2, far, cores), dma(2, far, cores), dma(far, cores), dma(far, cores),
        dma(far, far), dma(far, far), dma(cores), dma(cores), dma(1),
    ]
    vmem = pl.BlockSpec(memory_space=pltpu.VMEM)
    specs = [vmem] * 18
    specs[10] = pl.BlockSpec(memory_space=pl.ANY)
    return pl.pallas_call(
        functools.partial(layer_kernel, far, near, cores),
        out_shape=jax.ShapeDtypeStruct((rows, wide), bf16),
        in_specs=specs,
        out_specs=vmem,
        scratch_shapes=scratch,
        compiler_params=pltpu.CompilerParams(
            collective_id=0, has_side_effects=True, vmem_limit_bytes=60 * 1024 * 1024
        ),
    )(
        query_logits, value_rows, onward_forget_logits, reverse_forget_logits, output_gate_logits,
        onward_floor_gap[None], reverse_floor_gap[None], extra_log_decay, per_head_gain[None],
        residual, output_matrix, inner_norm_gain[None], inner_norm_bias[None], gate_matrix,
        up_matrix, down_matrix, closing_norm_gain[None], closing_norm_bias[None],
    )


def solution(mesh):
    a, b = P("sp", "tp"), P("tp")
    placed = (a, a, a, a, a, b, b, a, P(), a, P(None, "tp"), b, b, a, a, P("tp", "sp"), b, b)
    return jax.shard_map(
        shards, mesh=mesh, in_specs=placed, out_specs=P("sp", "tp"), check_vma=False
    )
```

```python
import functools
import math

import jax
import jax.numpy as jnp
from jax import lax
from jax.experimental import pallas as pl
from jax.experimental.pallas import tpu as pltpu
from jax.sharding import PartitionSpec as P

highest = lax.Precision.HIGHEST
alpha_mix = 2.0**0.25
norm_eps = 1e-05
head_eps = 1e-06
bf16 = jnp.bfloat16
f32 = jnp.float32
MESH = pl.DeviceIdType.MESH
pieces = 2


def pick(table, at):
    out = jnp.int32(table[0])
    for i, value in enumerate(table[1:], 1):
        out = jnp.where(at == i, jnp.int32(value), out)
    return out


def across(x, w):
    return lax.dot_general(x, w, (((1,), (1,)), ((), ())), preferred_element_type=f32)


def silu(x):
    return x / (1.0 + jnp.exp(-x))


def layer_kernel(
    far, near, cores,
    q_ref, v_ref, f_ref, r_ref, og_ref, fg_ref, rg_ref, ex_ref, hg_ref, res_ref, om_ref, ig_ref,
    ib_ref, gate_ref, up_ref, down_ref, cg_ref, cb_ref, out_ref,
    wbuf, wsend, st_send, tot_send, st_recv, tot_recv, fs_send, ft_send, f_recv, ft_recv,
    b_send, b_recv, om_all, res_all, ig_all, ib_all, g_all, x_all, inner, dq, hid, ts_send,
    ts_recv, rs_send, rs_recv, fin_all, xs,
    deal_s, deal_r, ring_s, ring_r, half_r, s1_s, s1_r, s2_s, s2_r, s3_s, s3_r, tp_s, tp_r, ga_s, ga_r,
    ag_s, ag_r, d2_s, d2_r, ts_s, ts_r, rs_s, rs_r, fin_s, fin_r, own_s,
):
    rows = q_ref.shape[0]
    heads, width = ex_ref.shape[0], hg_ref.shape[1]
    units, deep = wbuf.shape[3:]
    chunk = st_send.shape[2]
    per_head = near // heads
    share = near // cores
    half = (units // 2 + 15) // 16 * 16
    n2 = near // 2
    me, core = lax.axis_index("sp"), lax.axis_index("tp")
    z, p = me // near, me % near

    ring = [i ^ (i >> 1) for i in range(near)]
    spot = [ring.index(i) for i in range(near)]
    right = pick([ring[(spot[i] + 1) % near] for i in range(near)], p)
    left = pick([ring[(spot[i] - 1) % near] for i in range(near)], p)

    def behind(sign, d):
        return pick([ring[(spot[i] - sign * d) % near] for i in range(near)], p)

    partners = [sorted((j for j in range(far) if j != i), key=lambda j: (abs(j - i), j != i ^ 1))
                for i in range(far)]
    order = [z] + [pick([partners[i][k] for i in range(far)], z) for k in range(far - 1)]

    def copy(src, dst, ssem, rsem, to):
        return pltpu.make_async_remote_copy(
            src_ref=src, dst_ref=dst, send_sem=ssem, recv_sem=rsem, device_id=to,
            device_id_type=MESH,
        )

    def start(c, when=None):
        if when is None:
            c.start()
        else:
            pl.when(when)(c.start)

    def sent(sem, ref):
        copy(ref, ref, sem, sem, mate(1)).wait_send()

    def came(sem, ref):
        copy(ref, ref, sem, sem, mate(1)).wait_recv()

    def landed(c, when=None):
        if when is None:
            c.wait_recv()
        else:
            pl.when(when)(c.wait_recv)

    def at(zz, pp):
        return (zz * near + pp, core)

    def mate(m):
        return (me, (core + m) % cores)

    f_recv[...] = jnp.zeros_like(f_recv)
    ft_recv[...] = jnp.zeros_like(ft_recv)

    barrier = pltpu.get_barrier_semaphore()
    peers = [at(z, (p + j) % near) for j in range(1, near)]
    peers += [at((z + j) % far, p) for j in range(1, far)]
    peers += [mate(m) for m in range(1, cores)]
    for peer in peers:
        pl.semaphore_signal(barrier, inc=1, device_id=peer, device_id_type=MESH)

    own_om = pltpu.make_async_copy(om_ref, om_all.at[core], own_s.at[0])
    own_om.start()
    for i, ref in enumerate((gate_ref, up_ref)):
        whole = ref[...].astype(f32).T
        for j in range(far):
            wsend[j, i] = whole[j * units : (j + 1) * units].astype(bf16)
    wbuf[p, z, 0] = wsend[z, 0]
    wbuf[p, z, 1] = wsend[z, 1]
    wbuf[p, z, 2] = down_ref[pl.ds(pl.multiple_of(z * units, 16), units), :]
    res_all[core] = res_ref[...]
    ig_all[core] = ig_ref[...]
    ib_all[core] = ib_ref[...]
    pl.semaphore_wait(barrier, len(peers))

    def deal_copy(g, peer, slot, e):
        if g < 2:
            src = wsend.at[peer, g]
        else:
            src = down_ref.at[pl.ds(pl.multiple_of(peer * units, 16), units), :]
        return copy(src, wbuf.at[p, slot, g], deal_s.at[0], deal_r.at[g, slot], at(peer, p))

    def deal(g, e):
        start(deal_copy(g, (z + e) % far, z, e), z + e < far)
        start(deal_copy(g, (z + far - e) % far, z, far + e), z >= e)

    def ring_copy(k, sign, d, block):
        side = 0 if sign > 0 else 1
        ref = wbuf.at[block, order[k % far], k // far]
        if d == n2:
            ref = ref.at[pl.ds(0, half), :] if side == 0 else ref.at[pl.ds(half, units - half), :]
        to = right if sign > 0 else left
        if d < n2:
            arrive = ring_r.at[side, d - 1, k]
        else:
            arrive = half_r.at[max(0, k - 2 * far + 1)]
        return copy(ref, ref, ring_s.at[0], arrive, at(z, to))

    def ring_start(k):
        if k % far:
            landed(deal_copy(k // far, order[k % far], order[k % far], 0))
        for sign in (1, -1):
            start(ring_copy(k, sign, 1, p))

    def ring_forward(k):
        for d in range(1, n2):
            for sign in (1, -1):
                block = behind(sign, d)
                landed(ring_copy(k, sign, d, block))
                start(ring_copy(k, sign, d + 1, block))

    def ring_done(k):
        came(half_r.at[k - 2 * far + 1], wbuf.at[0, 0, 2])

    g0, u0, d0 = 0, far, 2 * far
    for g in range(2):
        deal(g, 1)
    ring_start(g0)

    pairs = ((om_ref, om_all), (res_ref, res_all), (ig_ref, ig_all), (ib_ref, ib_all))

    def tp_copy(i, m):
        src, dst = pairs[i]
        return copy(src, dst.at[core], tp_s.at[i], tp_r.at[i], mate(m))

    for m in range(1, cores):
        for i in range(len(pairs)):
            start(tp_copy(i, m))


    t = lax.broadcasted_iota(jnp.int32, (rows, rows), 0)
    s = lax.broadcasted_iota(jnp.int32, (rows, rows), 1)
    lower, upper = s <= t, s >= t
    for h in range(heads):
        cols = slice(h * width, (h + 1) * width)
        q = silu(q_ref[:, cols].astype(f32))
        v = v_ref[:, cols]
        extra = jnp.broadcast_to(ex_ref[h : h + 1, :], (width, rows)).T
        scores = jnp.zeros((rows, rows), f32)
        for d, (raw_ref, gap_ref, tri) in enumerate(
            ((f_ref, fg_ref, lower), (r_ref, rg_ref, upper))
        ):
            raw = raw_ref[:, cols].astype(f32)
            key = gap_ref[:, cols] * (1.0 / (1.0 + jnp.exp(raw)))
            log = jnp.log1p(-key) + extra
            run = jnp.dot(tri.astype(f32), log, precision=highest, preferred_element_type=f32)
            last = run[rows - 1 :, :] if d == 0 else run[:1, :]
            qd = (q * jnp.exp(run)).astype(bf16)
            ki = (key * jnp.exp(-run)).astype(bf16)
            ks = (key * jnp.exp(last - run)).astype(bf16)
            scores = scores + jnp.where(tri, across(qd, ki), 0.0)
            dq[d, :, cols] = qd
            state = lax.dot_general(v, ks, (((0,), (0,)), ((), ())), preferred_element_type=f32)
            for i in range(per_head):
                st_send[h * per_head + i, d] = state[i * chunk : (i + 1) * chunk].astype(bf16)
                tot_send[h * per_head + i, d] = last
        inner[:, cols] = jnp.dot(scores.astype(bf16), v, preferred_element_type=f32)

    def plane_copy(i, j):
        src, dst = ((st_send, st_recv), (tot_send, tot_recv))[i]
        to = (p + j) % near
        return copy(src.at[to], dst.at[p], s1_s.at[i], s1_r.at[i], at(z, to))

    for j in range(1, near):
        for i in range(2):
            start(plane_copy(i, j))
    st_recv[p] = st_send[p]
    tot_recv[p] = tot_send[p]

    came(s1_r.at[0], st_recv.at[pl.ds(0, near - 1)])
    came(s1_r.at[1], tot_recv.at[pl.ds(0, near - 1)])

    prefix = [[None] * near, [None] * near]
    gone = [[None] * near, [None] * near]
    for d in range(2):
        state = jnp.zeros((chunk, width), f32)
        total = jnp.zeros((1, width), f32)
        for b in range(near) if d == 0 else reversed(range(near)):
            prefix[d][b], gone[d][b] = state, total
            step = tot_recv[b, d]
            state = state * jnp.exp(step) + st_recv[b, d].astype(f32)
            total = total + step
        fs_send[d] = state.astype(bf16)
        ft_send[d] = total

    def far_copy(i, d, e):
        src, dst = ((fs_send, f_recv), (ft_send, ft_recv))[i]
        to = (z + e) % far if d == 0 else (z + far - e) % far
        return copy(src.at[d], dst.at[d, e], s2_s.at[i], s2_r.at[i], at(to, p))

    def far_valid(d, e):
        return z + e < far if d == 0 else z >= e

    for e in range(1, far):
        for d in range(2):
            for i in range(2):
                start(far_copy(i, d, e), far_valid(d, e))

    ring_start(u0)

    came(s2_r.at[0], f_recv.at[0, pl.ds(1, far - 1)])
    came(s2_r.at[1], ft_recv.at[0, pl.ds(1, far - 1)])

    for d in range(2):
        enter = jnp.zeros((chunk, width), f32)
        for e in reversed(range(1, far)):
            enter = enter * jnp.exp(ft_recv[d, e]) + f_recv[d, e].astype(f32)
        for b in range(near):
            b_send[b, d] = (enter * jnp.exp(gone[d][b]) + prefix[d][b]).astype(bf16)

    def back_copy(j):
        to = (p + j) % near
        return copy(b_send.at[to], b_recv.at[p], s3_s.at[0], s3_r.at[0], at(z, to))

    for j in range(1, near):
        start(back_copy(j))
    b_recv[p] = b_send[p]

    deal(0, 2)
    deal(1, 2)
    ring_forward(g0)
    ring_start(g0 + 1)

    came(s3_r.at[0], b_recv.at[pl.ds(0, near - 1)])

    for h in range(heads):
        cols = slice(h * width, (h + 1) * width)
        mixed = inner[:, cols]
        for d in range(2):
            state = jnp.concatenate(
                [b_recv[h * per_head + i, d].astype(f32) for i in range(per_head)], axis=0
            ).astype(bf16)
            mixed = mixed + across(dq[d, :, cols], state)
        normed = (
            mixed
            * lax.rsqrt(jnp.mean(mixed * mixed, axis=1, keepdims=True) + head_eps)
            * hg_ref[...]
        )
        g_all[core, :, cols] = (normed * silu(og_ref[:, cols].astype(f32))).astype(bf16)

    for m in range(1, cores):
        start(copy(g_all.at[core], g_all.at[core], ga_s.at[0], ga_r.at[0], mate(m)))
    ring_forward(u0)
    ring_start(u0 + 1)
    own_om.wait()
    for i in range(len(pairs)):
        came(tp_r.at[i], pairs[i][1].at[pl.ds(0, cores - 1)])
    came(ga_r.at[0], g_all.at[pl.ds(0, cores - 1)])

    span = q_ref.shape[1]
    parts = []
    for b in range(cores):
        mixer = alpha_mix * res_all[b].astype(f32)
        for m in range(cores):
            mixer = mixer + jnp.dot(
                g_all[m], om_all[b, m * span : (m + 1) * span, :], preferred_element_type=f32
            )
        parts.append(mixer)
    wide = parts[0].shape[1]
    model = cores * wide
    mean = sum(jnp.sum(x, axis=1, keepdims=True) for x in parts) / model
    parts = [x - mean for x in parts]
    var = sum(jnp.sum(x * x, axis=1, keepdims=True) for x in parts) / model
    scale = lax.rsqrt(var + norm_eps)
    for b, x in enumerate(parts):
        x_all[z, b] = (x * scale * ig_all[b] + ib_all[b]).astype(bf16)

    part = rows // pieces

    def line_copy(sign, d, i, out):
        block = (z + far + ((1 if out else 0) - d) * sign) % far
        side = 0 if sign > 0 else 1
        ref = x_all.at[block, core, pl.ds(i * part, part), :]
        to = at((z + far + sign) % far, p)
        return copy(ref, ref, ag_s.at[side, d - 1, i], ag_r.at[side, d - 1, i], to)

    def line_out(sign, d):
        if sign > 0:
            return jnp.logical_and(z + 1 < far, z >= d - 1)
        return jnp.logical_and(z > 0, z + d - 1 < far)

    def line_in(sign, d):
        return z >= d if sign > 0 else z + d < far

    def line_share(sign, d, i, m):
        ref = x_all.at[(z + far - d * sign) % far, core, pl.ds(i * part, part), :]
        return copy(ref, ref, d2_s.at[0], d2_r.at[0], mate(m))

    def line_step(d, i):
        for sign in (1, -1):
            landed(line_copy(sign, d, i, False), line_in(sign, d))
            if d + 1 < far:
                start(line_copy(sign, d + 1, i, True), line_out(sign, d + 1))
            for m in range(1, cores):
                start(line_share(sign, d, i, m), line_in(sign, d))

    for i in range(pieces):
        for sign in (1, -1):
            start(line_copy(sign, 1, i, True), line_out(sign, 1))
    deal(0, 3)
    ring_start(g0 + 2)
    ring_forward(g0 + 1)
    ring_forward(u0 + 1)
    ring_start(u0 + 2)
    ring_forward(g0 + 2)
    for i in range(pieces):
        line_step(1, i)
    deal(1, 3)
    ring_start(g0 + 3)
    line_step(2, 0)
    deal(2, 1)
    ring_forward(u0 + 2)
    for i in range(1, pieces):
        line_step(2, i)
    ring_start(u0 + 3)
    ring_forward(g0 + 3)
    ring_start(d0)
    for i in range(pieces):
        line_step(3, i)
    deal(2, 2)
    deal(2, 3)
    ring_forward(u0 + 3)
    ring_forward(d0)
    ring_start(d0 + 1)
    came(d2_r.at[0], x_all.at[pl.ds(0, far - 1), pl.ds(0, cores - 1)])
    came(half_r.at[0], wbuf.at[0, :, pl.ds(0, 2)])

    step = 256
    for n0 in range(0, units, step):
        n1 = min(units, n0 + step)
        gate = up = 0.0
        for pp in range(near):
            spots = [(zz * near + pp) * deep for zz in range(far)]
            x = jnp.concatenate(
                [
                    jnp.concatenate(
                        [x_all[j, c // wide, :, c % wide : c % wide + deep] for c in spots], axis=1
                    )
                    for j in range(far)
                ],
                axis=0,
            )
            wg, wu = (
                jnp.concatenate([wbuf[pp, zz, i, n0:n1, :] for zz in range(far)], axis=1)
                for i in range(2)
            )
            gate = gate + across(x, wg)
            up = up + across(x, wu)
        hid[:, n0:n1] = (silu(gate) * up).astype(bf16)

    def sum_copy(k, m):
        return copy(
            ts_send.at[k, (core + m) % cores], ts_recv.at[k, m - 1], ts_s.at[0], ts_r.at[k],
            mate(m),
        )

    def reduce_copy(k, j):
        to = order[j + 1]
        return copy(
            rs_send.at[k, to], rs_recv.at[z, order[k]], rs_s.at[0], rs_r.at[0], at(to, p)
        )

    def down(k):
        zz = order[k]
        w = jnp.concatenate([wbuf[pp, zz, 2] for pp in range(near)], axis=1)
        y = jnp.dot(hid[...], w, preferred_element_type=f32).astype(bf16)
        for c in range(cores):
            ts_send[k, c] = y[:, c * share * deep : (c + 1) * share * deep]
        for m in range(1, cores):
            start(sum_copy(k, m))

    def reduce(k):
        total = ts_send[k, core].astype(f32)
        came(ts_r.at[k], ts_recv.at[k])
        for m in range(1, cores):
            total = total + ts_recv[k, m - 1].astype(f32)
        total = total.astype(bf16)
        for j in range(far):
            rs_send[k, j] = total[j * rows : (j + 1) * rows]
        for j in reversed(range(far - 1)):
            start(reduce_copy(k, j))
        rs_recv[z, order[k]] = rs_send[k, z]

    ring_start(d0 + 2)
    for k in range(far):
        ring_done(d0 + k)
        down(k)
        if k + 1 < far:
            ring_forward(d0 + k + 1)
        if k + 3 < far:
            ring_start(d0 + k + 3)
        reduce(k)

    came(rs_r.at[0], rs_recv.at[pl.ds(0, far - 1)])
    mine = [sum(rs_recv[src, zz].astype(f32) for src in range(far)) for zz in range(far)]
    fin_all[core] = jnp.concatenate(mine, axis=1).astype(bf16)

    for m in range(1, cores):
        start(copy(fin_all.at[core], fin_all.at[core], fin_s.at[0], fin_r.at[0], mate(m)))
    came(fin_r.at[0], fin_all.at[pl.ds(0, cores - 1)])
    feed = [fin_all[c].astype(f32) for c in range(cores)]
    whole = jnp.concatenate(
        [
            feed[pp // share][:, (zz * share + pp % share) * deep : (zz * share + pp % share + 1) * deep]
            for zz in range(far)
            for pp in range(near)
        ],
        axis=1,
    )
    parts = [
        alpha_mix * x_all[z, b].astype(f32) + whole[:, b * wide : (b + 1) * wide]
        for b in range(cores)
    ]
    mean = sum(jnp.sum(x, axis=1, keepdims=True) for x in parts) / model
    parts = [x - mean for x in parts]
    var = sum(jnp.sum(x * x, axis=1, keepdims=True) for x in parts) / model
    scale = lax.rsqrt(var + norm_eps)
    for b, x in enumerate(parts):
        xs[b] = x * scale
    out_ref[...] = (xs[core] * cg_ref[...] + cb_ref[...]).astype(bf16)

    sent(deal_s.at[0], wbuf.at[0, pl.ds(0, far - 1)])
    sent(ring_s.at[0], wbuf.at[pl.ds(0, near - 1)])
    for i in range(len(pairs)):
        sent(tp_s.at[i], pairs[i][1].at[pl.ds(0, cores - 1)])
    sent(s1_s.at[0], st_recv.at[pl.ds(0, near - 1)])
    sent(s1_s.at[1], tot_recv.at[pl.ds(0, near - 1)])
    sent(s2_s.at[0], f_recv.at[0, pl.ds(1, far - 1)])
    sent(s2_s.at[1], ft_recv.at[0, pl.ds(1, far - 1)])
    sent(s3_s.at[0], b_recv.at[pl.ds(0, near - 1)])
    sent(ga_s.at[0], g_all.at[pl.ds(0, cores - 1)])
    for d in range(1, far):
        for sign in (1, -1):
            for i in range(pieces):
                pl.when(line_out(sign, d))(line_copy(sign, d, i, True).wait_send)
    sent(d2_s.at[0], x_all.at[pl.ds(0, far - 1), pl.ds(0, cores - 1)])
    sent(ts_s.at[0], ts_recv)
    sent(rs_s.at[0], rs_recv.at[pl.ds(0, far - 1)])
    sent(fin_s.at[0], fin_all.at[pl.ds(0, cores - 1)])


def shards(
    query_logits, value_rows, onward_forget_logits, reverse_forget_logits, output_gate_logits,
    onward_floor_gap, reverse_floor_gap, extra_log_decay, per_head_gain, residual, output_matrix,
    inner_norm_gain, inner_norm_bias, gate_matrix, up_matrix, down_matrix,
    closing_norm_gain, closing_norm_bias,
):
    count, cores = lax.axis_size("sp"), lax.axis_size("tp")
    far = math.gcd(count, 4)
    near = count // far
    rows, span = query_logits.shape
    heads = extra_log_decay.shape[1]
    width = span // heads
    wide = residual.shape[1]
    units = gate_matrix.shape[1] // far
    deep = gate_matrix.shape[0]
    chunk = heads * width // near
    share = near // cores
    n2 = near // 2
    inner_rows = output_matrix.shape[0]
    vm = pltpu.VMEM
    dma = lambda *shape: pltpu.SemaphoreType.DMA(shape)
    scratch = [
        vm((near, far, 3, units, deep), bf16),
        vm((far, 2, units, deep), bf16),
        vm((near, 2, chunk, width), bf16), vm((near, 2, 1, width), f32),
        vm((near, 2, chunk, width), bf16), vm((near, 2, 1, width), f32),
        vm((2, chunk, width), bf16), vm((2, 1, width), f32),
        vm((2, far, chunk, width), bf16), vm((2, far, 1, width), f32),
        vm((near, 2, chunk, width), bf16), vm((near, 2, chunk, width), bf16),
        vm((cores, inner_rows, wide), bf16), vm((cores, rows, wide), bf16),
        vm((cores, 1, wide), f32), vm((cores, 1, wide), f32),
        vm((cores, rows, span), bf16), vm((far, cores, rows, wide), bf16),
        vm((rows, span), f32), vm((2, rows, span), bf16), vm((far * rows, units), bf16),
        vm((far, cores, far * rows, share * deep), bf16),
        vm((far, cores - 1, far * rows, share * deep), bf16),
        vm((far, far, rows, share * deep), bf16), vm((far, far, rows, share * deep), bf16),
        vm((cores, rows, far * share * deep), bf16), vm((cores, rows, wide), f32),
        dma(1), dma(3, far), dma(1), dma(2, n2 - 1, 3 * far), dma(far + 1),
        dma(2), dma(2), dma(2), dma(2), dma(1), dma(1), dma(4), dma(4), dma(1), dma(1),
        dma(2, far - 1, pieces), dma(2, far - 1, pieces), dma(1), dma(1), dma(1), dma(far),
        dma(1), dma(1), dma(1), dma(1), dma(1),
    ]
    vmem = pl.BlockSpec(memory_space=pltpu.VMEM)
    specs = [vmem] * 18
    specs[10] = pl.BlockSpec(memory_space=pl.ANY)
    return pl.pallas_call(
        functools.partial(layer_kernel, far, near, cores),
        out_shape=jax.ShapeDtypeStruct((rows, wide), bf16),
        in_specs=specs,
        out_specs=vmem,
        scratch_shapes=scratch,
        compiler_params=pltpu.CompilerParams(
            collective_id=0, has_side_effects=True, vmem_limit_bytes=60 * 1024 * 1024
        ),
    )(
        query_logits, value_rows, onward_forget_logits, reverse_forget_logits, output_gate_logits,
        onward_floor_gap[None], reverse_floor_gap[None], extra_log_decay.T, per_head_gain[None],
        residual, output_matrix, inner_norm_gain[None], inner_norm_bias[None], gate_matrix,
        up_matrix, down_matrix, closing_norm_gain[None], closing_norm_bias[None],
    )


def solution(mesh):
    a, b = P("sp", "tp"), P("tp")
    placed = (a, a, a, a, a, b, b, a, P(), a, P(None, "tp"), b, b, a, a, P("tp", "sp"), b, b)
    return jax.shard_map(
        shards, mesh=mesh, in_specs=placed, out_specs=P("sp", "tp"), check_vma=False
    )
```

```python
import functools
import math

import jax
import jax.numpy as jnp
from jax import lax
from jax.experimental import pallas as pl
from jax.experimental.pallas import tpu as pltpu
from jax.sharding import PartitionSpec as P

highest = lax.Precision.HIGHEST
alpha_mix = 2.0**0.25
norm_eps = 1e-05
head_eps = 1e-06
bf16 = jnp.bfloat16
f32 = jnp.float32
MESH = pl.DeviceIdType.MESH
pieces = 2


def pick(table, at):
    out = jnp.int32(table[0])
    for i, value in enumerate(table[1:], 1):
        out = jnp.where(at == i, jnp.int32(value), out)
    return out


def across(x, w):
    return lax.dot_general(x, w, (((1,), (1,)), ((), ())), preferred_element_type=f32)


def silu(x):
    return x / (1.0 + jnp.exp(-x))


def layer_kernel(
    far, near, cores,
    q_in, v_in, f_in, r_in, og_in, fg_in, rg_in, ex_in, hg_in, res_ref, om_ref, ig_ref, ib_ref,
    gate_in, up_in, down_ref, cg_in, cb_in, out_ref,
    q_ref, v_ref, f_ref, r_ref, og_ref, fg_ref, rg_ref, ex_ref, hg_ref, gate_ref, up_ref, cg_ref,
    cb_ref,
    wbuf, wsend, st_send, tot_send, st_recv, tot_recv, fs_send, ft_send, f_recv, ft_recv,
    b_send, b_recv, om_all, res_all, ig_all, ib_all, g_all, x_all, inner, dq, hid, ts_send,
    ts_recv, rs_send, rs_recv, fin_all, xs,
    deal_s, deal_r, ring_s, ring_r, half_r, s1_s, s1_r, s2_s, s2_r, s3_s, s3_r, tp_s, tp_r, ga_s, ga_r,
    ag_s, ag_r, d2_s, d2_r, ts_s, ts_r, rs_s, rs_r, fin_s, fin_r, load_s,
):
    rows = q_in.shape[0]
    heads, width = ex_in.shape[0], hg_in.shape[1]
    units, deep = wbuf.shape[3:]
    chunk = st_send.shape[2]
    per_head = near // heads
    share = near // cores
    half = (units // 2 + 15) // 16 * 16
    n2 = near // 2
    me, core = lax.axis_index("sp"), lax.axis_index("tp")
    z, p = me // near, me % near

    ring = [i ^ (i >> 1) for i in range(near)]
    spot = [ring.index(i) for i in range(near)]
    right = pick([ring[(spot[i] + 1) % near] for i in range(near)], p)
    left = pick([ring[(spot[i] - 1) % near] for i in range(near)], p)

    def behind(sign, d):
        return pick([ring[(spot[i] - sign * d) % near] for i in range(near)], p)

    partners = [sorted((j for j in range(far) if j != i), key=lambda j: (abs(j - i), j != i ^ 1))
                for i in range(far)]
    order = [z] + [pick([partners[i][k] for i in range(far)], z) for k in range(far - 1)]

    def copy(src, dst, ssem, rsem, to):
        return pltpu.make_async_remote_copy(
            src_ref=src, dst_ref=dst, send_sem=ssem, recv_sem=rsem, device_id=to,
            device_id_type=MESH,
        )

    def start(c, when=None):
        if when is None:
            c.start()
        else:
            pl.when(when)(c.start)

    def sent(sem, ref):
        copy(ref, ref, sem, sem, mate(1)).wait_send()

    def came(sem, ref):
        copy(ref, ref, sem, sem, mate(1)).wait_recv()

    def landed(c, when=None):
        if when is None:
            c.wait_recv()
        else:
            pl.when(when)(c.wait_recv)

    def at(zz, pp):
        return (zz * near + pp, core)

    def mate(m):
        return (me, (core + m) % cores)

    down_own = down_ref.at[pl.ds(pl.multiple_of(z * units, 16), units), :]
    loads = {}
    for name, src, dst in (
        ("gate", gate_in, gate_ref), ("up", up_in, up_ref), ("f", f_in, f_ref),
        ("r", r_in, r_ref), ("fg", fg_in, fg_ref), ("rg", rg_in, rg_ref), ("ex", ex_in, ex_ref),
        ("q", q_in, q_ref), ("v", v_in, v_ref), ("down", down_own, wbuf.at[p, z, 2]),
        ("om", om_ref, om_all.at[core]), ("res", res_ref, res_all.at[core]),
        ("ig", ig_ref, ig_all.at[core]), ("ib", ib_ref, ib_all.at[core]), ("og", og_in, og_ref),
        ("hg", hg_in, hg_ref), ("cg", cg_in, cg_ref), ("cb", cb_in, cb_ref),
    ):
        loads[name] = pltpu.make_async_copy(src, dst, load_s.at[len(loads)])

    def loaded(*names):
        for name in names:
            loads[name].wait()

    f_recv[...] = jnp.zeros_like(f_recv)
    ft_recv[...] = jnp.zeros_like(ft_recv)

    barrier = pltpu.get_barrier_semaphore()
    peers = [at(z, (p + j) % near) for j in range(1, near)]
    peers += [at((z + j) % far, p) for j in range(1, far)]
    peers += [mate(m) for m in range(1, cores)]
    for peer in peers:
        pl.semaphore_signal(barrier, inc=1, device_id=peer, device_id_type=MESH)

    for load in loads.values():
        load.start()
    loaded("gate", "up")
    for i, ref in enumerate((gate_ref, up_ref)):
        whole = ref[...].astype(f32).T
        for j in range(far):
            wsend[j, i] = whole[j * units : (j + 1) * units].astype(bf16)
    wbuf[p, z, 0] = wsend[z, 0]
    wbuf[p, z, 1] = wsend[z, 1]
    pl.semaphore_wait(barrier, len(peers))

    def deal_copy(g, peer, slot, e):
        if g < 2:
            src = wsend.at[peer, g]
        else:
            src = down_ref.at[pl.ds(pl.multiple_of(peer * units, 16), units), :]
        return copy(src, wbuf.at[p, slot, g], deal_s.at[0], deal_r.at[g, slot], at(peer, p))

    def deal(g, e):
        start(deal_copy(g, (z + e) % far, z, e), z + e < far)
        start(deal_copy(g, (z + far - e) % far, z, far + e), z >= e)

    def ring_copy(k, sign, d, block):
        side = 0 if sign > 0 else 1
        ref = wbuf.at[block, order[k % far], k // far]
        if d == n2:
            ref = ref.at[pl.ds(0, half), :] if side == 0 else ref.at[pl.ds(half, units - half), :]
        to = right if sign > 0 else left
        if d < n2:
            arrive = ring_r.at[side, d - 1, k]
        else:
            arrive = half_r.at[max(0, k - 2 * far + 1)]
        return copy(ref, ref, ring_s.at[0], arrive, at(z, to))

    def ring_start(k):
        if k % far:
            landed(deal_copy(k // far, order[k % far], order[k % far], 0))
        for sign in (1, -1):
            start(ring_copy(k, sign, 1, p))

    def ring_forward(k):
        for d in range(1, n2):
            for sign in (1, -1):
                block = behind(sign, d)
                landed(ring_copy(k, sign, d, block))
                start(ring_copy(k, sign, d + 1, block))

    def ring_done(k):
        came(half_r.at[k - 2 * far + 1], wbuf.at[0, 0, 2])

    g0, u0, d0 = 0, far, 2 * far
    for g in range(2):
        deal(g, 1)
    ring_start(g0)

    pairs = ((om_ref, om_all), (res_ref, res_all), (ig_ref, ig_all), (ib_ref, ib_all))

    def tp_copy(i, m):
        src, dst = pairs[i]
        return copy(src, dst.at[core], tp_s.at[i], tp_r.at[i], mate(m))

    for m in range(1, cores):
        for i in range(len(pairs)):
            start(tp_copy(i, m))


    loaded("f", "r", "fg", "rg", "ex", "q", "v")
    t = lax.broadcasted_iota(jnp.int32, (rows, rows), 0)
    s = lax.broadcasted_iota(jnp.int32, (rows, rows), 1)
    lower, upper = s <= t, s >= t
    for h in range(heads):
        cols = slice(h * width, (h + 1) * width)
        q = silu(q_ref[:, cols].astype(f32))
        v = v_ref[:, cols]
        extra = jnp.broadcast_to(ex_ref[h : h + 1, :], (width, rows)).T
        scores = jnp.zeros((rows, rows), f32)
        for d, (raw_ref, gap_ref, tri) in enumerate(
            ((f_ref, fg_ref, lower), (r_ref, rg_ref, upper))
        ):
            raw = raw_ref[:, cols].astype(f32)
            key = gap_ref[:, cols] * (1.0 / (1.0 + jnp.exp(raw)))
            log = jnp.log1p(-key) + extra
            run = jnp.dot(tri.astype(f32), log, precision=highest, preferred_element_type=f32)
            last = run[rows - 1 :, :] if d == 0 else run[:1, :]
            qd = (q * jnp.exp(run)).astype(bf16)
            ki = (key * jnp.exp(-run)).astype(bf16)
            ks = (key * jnp.exp(last - run)).astype(bf16)
            scores = scores + jnp.where(tri, across(qd, ki), 0.0)
            dq[d, :, cols] = qd
            state = lax.dot_general(v, ks, (((0,), (0,)), ((), ())), preferred_element_type=f32)
            for i in range(per_head):
                st_send[h * per_head + i, d] = state[i * chunk : (i + 1) * chunk].astype(bf16)
                tot_send[h * per_head + i, d] = last
        inner[:, cols] = jnp.dot(scores.astype(bf16), v, preferred_element_type=f32)

    def plane_copy(i, j):
        src, dst = ((st_send, st_recv), (tot_send, tot_recv))[i]
        to = (p + j) % near
        return copy(src.at[to], dst.at[p], s1_s.at[i], s1_r.at[i], at(z, to))

    for j in range(1, near):
        for i in range(2):
            start(plane_copy(i, j))
    st_recv[p] = st_send[p]
    tot_recv[p] = tot_send[p]

    came(s1_r.at[0], st_recv.at[pl.ds(0, near - 1)])
    came(s1_r.at[1], tot_recv.at[pl.ds(0, near - 1)])

    prefix = [[None] * near, [None] * near]
    gone = [[None] * near, [None] * near]
    for d in range(2):
        state = jnp.zeros((chunk, width), f32)
        total = jnp.zeros((1, width), f32)
        for b in range(near) if d == 0 else reversed(range(near)):
            prefix[d][b], gone[d][b] = state, total
            step = tot_recv[b, d]
            state = state * jnp.exp(step) + st_recv[b, d].astype(f32)
            total = total + step
        fs_send[d] = state.astype(bf16)
        ft_send[d] = total

    def far_copy(i, d, e):
        src, dst = ((fs_send, f_recv), (ft_send, ft_recv))[i]
        to = (z + e) % far if d == 0 else (z + far - e) % far
        return copy(src.at[d], dst.at[d, e], s2_s.at[i], s2_r.at[i], at(to, p))

    def far_valid(d, e):
        return z + e < far if d == 0 else z >= e

    for e in range(1, far):
        for d in range(2):
            for i in range(2):
                start(far_copy(i, d, e), far_valid(d, e))

    ring_start(u0)

    came(s2_r.at[0], f_recv.at[0, pl.ds(1, far - 1)])
    came(s2_r.at[1], ft_recv.at[0, pl.ds(1, far - 1)])

    for d in range(2):
        enter = jnp.zeros((chunk, width), f32)
        for e in reversed(range(1, far)):
            enter = enter * jnp.exp(ft_recv[d, e]) + f_recv[d, e].astype(f32)
        for b in range(near):
            b_send[b, d] = (enter * jnp.exp(gone[d][b]) + prefix[d][b]).astype(bf16)

    def back_copy(j):
        to = (p + j) % near
        return copy(b_send.at[to], b_recv.at[p], s3_s.at[0], s3_r.at[0], at(z, to))

    for j in range(1, near):
        start(back_copy(j))
    b_recv[p] = b_send[p]

    deal(0, 2)
    deal(1, 2)
    ring_forward(g0)
    ring_start(g0 + 1)

    came(s3_r.at[0], b_recv.at[pl.ds(0, near - 1)])

    loaded("og", "hg")
    for h in range(heads):
        cols = slice(h * width, (h + 1) * width)
        mixed = inner[:, cols]
        for d in range(2):
            state = jnp.concatenate(
                [b_recv[h * per_head + i, d].astype(f32) for i in range(per_head)], axis=0
            ).astype(bf16)
            mixed = mixed + across(dq[d, :, cols], state)
        normed = (
            mixed
            * lax.rsqrt(jnp.mean(mixed * mixed, axis=1, keepdims=True) + head_eps)
            * hg_ref[...]
        )
        g_all[core, :, cols] = (normed * silu(og_ref[:, cols].astype(f32))).astype(bf16)

    for m in range(1, cores):
        start(copy(g_all.at[core], g_all.at[core], ga_s.at[0], ga_r.at[0], mate(m)))
    ring_forward(u0)
    ring_start(u0 + 1)
    loaded("om", "res", "ig", "ib")
    for i in range(len(pairs)):
        came(tp_r.at[i], pairs[i][1].at[pl.ds(0, cores - 1)])
    came(ga_r.at[0], g_all.at[pl.ds(0, cores - 1)])

    span = q_ref.shape[1]
    parts = []
    for b in range(cores):
        mixer = alpha_mix * res_all[b].astype(f32)
        for m in range(cores):
            mixer = mixer + jnp.dot(
                g_all[m], om_all[b, m * span : (m + 1) * span, :], preferred_element_type=f32
            )
        parts.append(mixer)
    wide = parts[0].shape[1]
    model = cores * wide
    mean = sum(jnp.sum(x, axis=1, keepdims=True) for x in parts) / model
    parts = [x - mean for x in parts]
    var = sum(jnp.sum(x * x, axis=1, keepdims=True) for x in parts) / model
    scale = lax.rsqrt(var + norm_eps)
    for b, x in enumerate(parts):
        x_all[z, b] = (x * scale * ig_all[b] + ib_all[b]).astype(bf16)

    part = rows // pieces

    def line_copy(sign, d, i, out):
        block = (z + far + ((1 if out else 0) - d) * sign) % far
        side = 0 if sign > 0 else 1
        ref = x_all.at[block, core, pl.ds(i * part, part), :]
        to = at((z + far + sign) % far, p)
        return copy(ref, ref, ag_s.at[side, d - 1, i], ag_r.at[side, d - 1, i], to)

    def line_out(sign, d):
        if sign > 0:
            return jnp.logical_and(z + 1 < far, z >= d - 1)
        return jnp.logical_and(z > 0, z + d - 1 < far)

    def line_in(sign, d):
        return z >= d if sign > 0 else z + d < far

    def line_share(sign, d, i, m):
        ref = x_all.at[(z + far - d * sign) % far, core, pl.ds(i * part, part), :]
        return copy(ref, ref, d2_s.at[0], d2_r.at[0], mate(m))

    def line_step(d, i):
        for sign in (1, -1):
            landed(line_copy(sign, d, i, False), line_in(sign, d))
            if d + 1 < far:
                start(line_copy(sign, d + 1, i, True), line_out(sign, d + 1))
            for m in range(1, cores):
                start(line_share(sign, d, i, m), line_in(sign, d))

    for i in range(pieces):
        for sign in (1, -1):
            start(line_copy(sign, 1, i, True), line_out(sign, 1))
    deal(0, 3)
    ring_start(g0 + 2)
    ring_forward(g0 + 1)
    ring_forward(u0 + 1)
    ring_start(u0 + 2)
    ring_forward(g0 + 2)
    for i in range(pieces):
        line_step(1, i)
    deal(1, 3)
    ring_start(g0 + 3)
    line_step(2, 0)
    ring_forward(u0 + 2)
    for i in range(1, pieces):
        line_step(2, i)
    deal(2, 1)
    ring_start(u0 + 3)
    ring_forward(g0 + 3)
    ring_forward(u0 + 3)
    loaded("down")
    ring_start(d0)
    for i in range(pieces):
        line_step(3, i)
    deal(2, 2)
    deal(2, 3)
    ring_start(d0 + 1)
    came(d2_r.at[0], x_all.at[pl.ds(0, far - 1), pl.ds(0, cores - 1)])
    came(half_r.at[0], wbuf.at[0, :, pl.ds(0, 2)])

    step = 256
    for n0 in range(0, units, step):
        n1 = min(units, n0 + step)
        gate = up = 0.0
        for pp in range(near):
            spots = [(zz * near + pp) * deep for zz in range(far)]
            x = jnp.concatenate(
                [
                    jnp.concatenate(
                        [x_all[j, c // wide, :, c % wide : c % wide + deep] for c in spots], axis=1
                    )
                    for j in range(far)
                ],
                axis=0,
            )
            wg, wu = (
                jnp.concatenate([wbuf[pp, zz, i, n0:n1, :] for zz in range(far)], axis=1)
                for i in range(2)
            )
            gate = gate + across(x, wg)
            up = up + across(x, wu)
        hid[:, n0:n1] = (silu(gate) * up).astype(bf16)

    close = [p] + [behind(sign, d) for d in range(1, n2) for sign in (1, -1)]
    opposite = behind(1, n2)

    def sum_copy(k, pp):
        owner = pp // share
        dst = ts_recv.at[k, pp % share, (owner + cores - 1 - core) % cores]
        return copy(ts_send.at[k, pp], dst, ts_s.at[0], ts_r.at[k, pp % share], (me, owner))

    def down(k, slots):
        w = jnp.concatenate([wbuf[pp, order[k], 2] for pp in slots], axis=1)
        y = jnp.dot(hid[...], w, preferred_element_type=f32).astype(bf16)
        for i, pp in enumerate(slots):
            ts_send[k, pp] = y[:, i * deep : (i + 1) * deep]
        for pp in slots:
            start(sum_copy(k, pp), pp // share != core)

    def reduce_copy(k, i, j):
        to = order[j + 1]
        dst = rs_recv.at[z, order[k], i]
        return copy(rs_send.at[k, i, to], dst, rs_s.at[0], rs_r.at[0], at(to, p))

    def reduce_slot(k, i):
        total = ts_send[k, core * share + i].astype(f32)
        came(ts_r.at[k, i], ts_recv.at[k, i])
        for m in range(cores - 1):
            total = total + ts_recv[k, i, m].astype(f32)
        total = total.astype(bf16)
        for j in range(far):
            rs_send[k, i, j] = total[j * rows : (j + 1) * rows]
        for j in reversed(range(far - 1)):
            start(reduce_copy(k, i, j))
        rs_recv[z, order[k], i] = rs_send[k, i, z]

    def reduce(k, late):
        for i in range(share):
            mine_late = core * share + i == opposite
            when = mine_late if late else jnp.logical_not(mine_late)
            pl.when(when)(functools.partial(reduce_slot, k, i))

    for k in range(far):
        ring_forward(d0 + k)
        down(k, close)
        if k:
            ring_done(d0 + k - 1)
            down(k - 1, [opposite])
        reduce(k, False)
        if k:
            reduce(k - 1, True)
        if k + 2 < far:
            ring_start(d0 + k + 2)
    ring_done(d0 + far - 1)
    down(far - 1, [opposite])
    reduce(far - 1, True)

    came(rs_r.at[0], rs_recv.at[pl.ds(0, far - 1)])
    mine = [
        sum(rs_recv[src, zz, i].astype(f32) for src in range(far))
        for zz in range(far)
        for i in range(share)
    ]
    fin_all[core] = jnp.concatenate(mine, axis=1).astype(bf16)

    for m in range(1, cores):
        start(copy(fin_all.at[core], fin_all.at[core], fin_s.at[0], fin_r.at[0], mate(m)))
    came(fin_r.at[0], fin_all.at[pl.ds(0, cores - 1)])
    loaded("cg", "cb")
    feed = [fin_all[c].astype(f32) for c in range(cores)]
    whole = jnp.concatenate(
        [
            feed[pp // share][:, (zz * share + pp % share) * deep : (zz * share + pp % share + 1) * deep]
            for zz in range(far)
            for pp in range(near)
        ],
        axis=1,
    )
    parts = [
        alpha_mix * x_all[z, b].astype(f32) + whole[:, b * wide : (b + 1) * wide]
        for b in range(cores)
    ]
    mean = sum(jnp.sum(x, axis=1, keepdims=True) for x in parts) / model
    parts = [x - mean for x in parts]
    var = sum(jnp.sum(x * x, axis=1, keepdims=True) for x in parts) / model
    scale = lax.rsqrt(var + norm_eps)
    for b, x in enumerate(parts):
        xs[b] = x * scale
    out_ref[...] = (xs[core] * cg_ref[...] + cb_ref[...]).astype(bf16)

    sent(deal_s.at[0], wbuf.at[0, pl.ds(0, far - 1)])
    sent(ring_s.at[0], wbuf.at[pl.ds(0, near - 1)])
    for i in range(len(pairs)):
        sent(tp_s.at[i], pairs[i][1].at[pl.ds(0, cores - 1)])
    sent(s1_s.at[0], st_recv.at[pl.ds(0, near - 1)])
    sent(s1_s.at[1], tot_recv.at[pl.ds(0, near - 1)])
    sent(s2_s.at[0], f_recv.at[0, pl.ds(1, far - 1)])
    sent(s2_s.at[1], ft_recv.at[0, pl.ds(1, far - 1)])
    sent(s3_s.at[0], b_recv.at[pl.ds(0, near - 1)])
    sent(ga_s.at[0], g_all.at[pl.ds(0, cores - 1)])
    for d in range(1, far):
        for sign in (1, -1):
            for i in range(pieces):
                pl.when(line_out(sign, d))(line_copy(sign, d, i, True).wait_send)
    sent(d2_s.at[0], x_all.at[pl.ds(0, far - 1), pl.ds(0, cores - 1)])
    sent(ts_s.at[0], ts_send.at[:, pl.ds(0, near - share)])
    sent(rs_s.at[0], rs_send.at[:, :, pl.ds(0, far - 1)])
    sent(fin_s.at[0], fin_all.at[pl.ds(0, cores - 1)])


def shards(
    query_logits, value_rows, onward_forget_logits, reverse_forget_logits, output_gate_logits,
    onward_floor_gap, reverse_floor_gap, extra_log_decay, per_head_gain, residual, output_matrix,
    inner_norm_gain, inner_norm_bias, gate_matrix, up_matrix, down_matrix,
    closing_norm_gain, closing_norm_bias,
):
    count, cores = lax.axis_size("sp"), lax.axis_size("tp")
    far = math.gcd(count, 4)
    near = count // far
    rows, span = query_logits.shape
    heads = extra_log_decay.shape[1]
    width = span // heads
    wide = residual.shape[1]
    units = gate_matrix.shape[1] // far
    deep = gate_matrix.shape[0]
    chunk = heads * width // near
    share = near // cores
    n2 = near // 2
    inner_rows = output_matrix.shape[0]
    vm = pltpu.VMEM
    dma = lambda *shape: pltpu.SemaphoreType.DMA(shape)
    scratch = [
        vm((rows, span), bf16), vm((rows, span), bf16), vm((rows, span), bf16),
        vm((rows, span), bf16), vm((rows, span), bf16), vm((1, span), f32), vm((1, span), f32),
        vm((heads, rows), f32), vm((1, width), f32), vm(gate_matrix.shape, bf16),
        vm(gate_matrix.shape, bf16), vm((1, wide), f32), vm((1, wide), f32),
        vm((near, far, 3, units, deep), bf16),
        vm((far, 2, units, deep), bf16),
        vm((near, 2, chunk, width), bf16), vm((near, 2, 1, width), f32),
        vm((near, 2, chunk, width), bf16), vm((near, 2, 1, width), f32),
        vm((2, chunk, width), bf16), vm((2, 1, width), f32),
        vm((2, far, chunk, width), bf16), vm((2, far, 1, width), f32),
        vm((near, 2, chunk, width), bf16), vm((near, 2, chunk, width), bf16),
        vm((cores, inner_rows, wide), bf16), vm((cores, rows, wide), bf16),
        vm((cores, 1, wide), f32), vm((cores, 1, wide), f32),
        vm((cores, rows, span), bf16), vm((far, cores, rows, wide), bf16),
        vm((rows, span), f32), vm((2, rows, span), bf16), vm((far * rows, units), bf16),
        vm((far, near, far * rows, deep), bf16), vm((far, share, cores - 1, far * rows, deep), bf16),
        vm((far, share, far, rows, deep), bf16), vm((far, far, share, rows, deep), bf16),
        vm((cores, rows, far * share * deep), bf16), vm((cores, rows, wide), f32),
        dma(1), dma(3, far), dma(1), dma(2, n2 - 1, 3 * far), dma(far + 1),
        dma(2), dma(2), dma(2), dma(2), dma(1), dma(1), dma(4), dma(4), dma(1), dma(1),
        dma(2, far - 1, pieces), dma(2, far - 1, pieces), dma(1), dma(1), dma(1), dma(far, share),
        dma(1), dma(1), dma(1), dma(1), dma(18),
    ]
    vmem = pl.BlockSpec(memory_space=pltpu.VMEM)
    specs = [pl.BlockSpec(memory_space=pl.ANY)] * 18
    return pl.pallas_call(
        functools.partial(layer_kernel, far, near, cores),
        out_shape=jax.ShapeDtypeStruct((rows, wide), bf16),
        in_specs=specs,
        out_specs=vmem,
        scratch_shapes=scratch,
        compiler_params=pltpu.CompilerParams(
            collective_id=0, has_side_effects=True, vmem_limit_bytes=60 * 1024 * 1024
        ),
    )(
        query_logits, value_rows, onward_forget_logits, reverse_forget_logits, output_gate_logits,
        onward_floor_gap[None], reverse_floor_gap[None], extra_log_decay.T, per_head_gain[None],
        residual, output_matrix, inner_norm_gain[None], inner_norm_bias[None], gate_matrix,
        up_matrix, down_matrix, closing_norm_gain[None], closing_norm_bias[None],
    )


def solution(mesh):
    a, b = P("sp", "tp"), P("tp")
    placed = (a, a, a, a, a, b, b, a, P(), a, P(None, "tp"), b, b, a, a, P("tp", "sp"), b, b)
    return jax.shard_map(
        shards, mesh=mesh, in_specs=placed, out_specs=P("sp", "tp"), check_vma=False
    )
```

```python
import functools
import math

import jax
import jax.numpy as jnp
from jax import lax
from jax.experimental import pallas as pl
from jax.experimental.pallas import tpu as pltpu
from jax.sharding import PartitionSpec as P

highest = lax.Precision.HIGHEST
alpha_mix = 2.0**0.25
norm_eps = 1e-05
head_eps = 1e-06
bf16 = jnp.bfloat16
f32 = jnp.float32
MESH = pl.DeviceIdType.MESH
pieces = 2


def pick(table, at):
    out = jnp.int32(table[0])
    for i, value in enumerate(table[1:], 1):
        out = jnp.where(at == i, jnp.int32(value), out)
    return out


def across(x, w):
    return lax.dot_general(x, w, (((1,), (1,)), ((), ())), preferred_element_type=f32)


def silu(x):
    return x / (1.0 + jnp.exp(-x))


def layer_kernel(
    far, near, cores,
    q_in, v_in, f_in, r_in, og_in, fg_in, rg_in, ex_in, hg_in, res_ref, om_ref, ig_ref, ib_ref,
    gate_in, up_in, down_ref, cg_in, cb_in, out_ref,
    q_ref, v_ref, f_ref, r_ref, og_ref, fg_ref, rg_ref, ex_ref, hg_ref, gate_ref, up_ref, cg_ref,
    cb_ref,
    wbuf, wsend, st_send, tot_send, st_recv, tot_recv, fs_send, ft_send, f_recv, ft_recv,
    b_send, b_recv, om_all, res_all, ig_all, ib_all, g_all, x_all, inner, dq, hid, ts_send,
    ts_recv, rs_send, rs_recv, fin_all, xs,
    deal_s, deal_r, ring_s, ring_r, half_r, s1_s, s1_r, s2_s, s2_r, s3_s, s3_r, tp_s, tp_r, ga_s, ga_r,
    ag_s, ag_r, d2_s, d2_r, ts_s, ts_r, rs_s, rs_r, fin_s, fin_r, load_s,
):
    rows = q_in.shape[0]
    heads, width = ex_in.shape[0], hg_in.shape[1]
    units, deep = wbuf.shape[3:]
    chunk = st_send.shape[2]
    per_head = near // heads
    share = near // cores
    half = (units // 2 + 15) // 16 * 16
    n2 = near // 2
    me, core = lax.axis_index("sp"), lax.axis_index("tp")
    z, p = me // near, me % near

    ring = [i ^ (i >> 1) for i in range(near)]
    spot = [ring.index(i) for i in range(near)]
    right = pick([ring[(spot[i] + 1) % near] for i in range(near)], p)
    left = pick([ring[(spot[i] - 1) % near] for i in range(near)], p)

    def behind(sign, d):
        return pick([ring[(spot[i] - sign * d) % near] for i in range(near)], p)

    partners = [sorted((j for j in range(far) if j != i), key=lambda j: (abs(j - i), j != i ^ 1))
                for i in range(far)]
    order = [z] + [pick([partners[i][k] for i in range(far)], z) for k in range(far - 1)]

    def copy(src, dst, ssem, rsem, to):
        return pltpu.make_async_remote_copy(
            src_ref=src, dst_ref=dst, send_sem=ssem, recv_sem=rsem, device_id=to,
            device_id_type=MESH,
        )

    def start(c, when=None):
        if when is None:
            c.start()
        else:
            pl.when(when)(c.start)

    def sent(sem, ref):
        copy(ref, ref, sem, sem, mate(1)).wait_send()

    def came(sem, ref):
        copy(ref, ref, sem, sem, mate(1)).wait_recv()

    def landed(c, when=None):
        if when is None:
            c.wait_recv()
        else:
            pl.when(when)(c.wait_recv)

    def at(zz, pp):
        return (zz * near + pp, core)

    def mate(m):
        return (me, (core + m) % cores)

    down_own = down_ref.at[pl.ds(pl.multiple_of(z * units, 16), units), :]
    loads = {}
    for name, src, dst in (
        ("gate", gate_in, gate_ref), ("up", up_in, up_ref), ("f", f_in, f_ref),
        ("r", r_in, r_ref), ("fg", fg_in, fg_ref), ("rg", rg_in, rg_ref), ("ex", ex_in, ex_ref),
        ("q", q_in, q_ref), ("v", v_in, v_ref), ("down", down_own, wbuf.at[p, z, 2]),
        ("om", om_ref, om_all.at[core]), ("res", res_ref, res_all.at[core]),
        ("ig", ig_ref, ig_all.at[core]), ("ib", ib_ref, ib_all.at[core]), ("og", og_in, og_ref),
        ("hg", hg_in, hg_ref), ("cg", cg_in, cg_ref), ("cb", cb_in, cb_ref),
    ):
        loads[name] = pltpu.make_async_copy(src, dst, load_s.at[len(loads)])

    def loaded(*names):
        for name in names:
            loads[name].wait()

    f_recv[...] = jnp.zeros_like(f_recv)
    ft_recv[...] = jnp.zeros_like(ft_recv)

    barrier = pltpu.get_barrier_semaphore()
    peers = [at(z, (p + j) % near) for j in range(1, near)]
    peers += [at((z + j) % far, p) for j in range(1, far)]
    peers += [mate(m) for m in range(1, cores)]
    for peer in peers:
        pl.semaphore_signal(barrier, inc=1, device_id=peer, device_id_type=MESH)

    for load in loads.values():
        load.start()
    def turn(i, ref):
        whole = ref[...].astype(f32).T
        for j in range(far):
            wsend[j, i] = whole[j * units : (j + 1) * units].astype(bf16)
        wbuf[p, z, i] = wsend[z, i]

    loaded("gate")
    turn(0, gate_ref)
    pl.semaphore_wait(barrier, len(peers))

    def deal_copy(g, peer, slot, e):
        if g < 2:
            src = wsend.at[peer, g]
        else:
            src = down_ref.at[pl.ds(pl.multiple_of(peer * units, 16), units), :]
        return copy(src, wbuf.at[p, slot, g], deal_s.at[0], deal_r.at[g, slot], at(peer, p))

    def deal(g, e):
        start(deal_copy(g, (z + e) % far, z, e), z + e < far)
        start(deal_copy(g, (z + far - e) % far, z, far + e), z >= e)

    def ring_copy(k, sign, d, block):
        side = 0 if sign > 0 else 1
        ref = wbuf.at[block, order[k % far], k // far]
        if d == n2:
            ref = ref.at[pl.ds(0, half), :] if side == 0 else ref.at[pl.ds(half, units - half), :]
        to = right if sign > 0 else left
        if d < n2:
            arrive = ring_r.at[side, d - 1, k]
        else:
            arrive = half_r.at[max(0, k - 2 * far + 1)]
        return copy(ref, ref, ring_s.at[0], arrive, at(z, to))

    def ring_start(k):
        if k % far:
            landed(deal_copy(k // far, order[k % far], order[k % far], 0))
        for sign in (1, -1):
            start(ring_copy(k, sign, 1, p))

    def ring_forward(k):
        for d in range(1, n2):
            for sign in (1, -1):
                block = behind(sign, d)
                landed(ring_copy(k, sign, d, block))
                start(ring_copy(k, sign, d + 1, block))

    def ring_done(k):
        came(half_r.at[k - 2 * far + 1], wbuf.at[0, 0, 2])

    g0, u0, d0 = 0, far, 2 * far
    deal(0, 1)
    ring_start(g0)
    loaded("up")
    turn(1, up_ref)
    deal(1, 1)

    pairs = ((om_ref, om_all), (res_ref, res_all), (ig_ref, ig_all), (ib_ref, ib_all))

    def tp_copy(i, m):
        src, dst = pairs[i]
        return copy(src, dst.at[core], tp_s.at[i], tp_r.at[i], mate(m))

    for m in range(1, cores):
        for i in range(len(pairs)):
            start(tp_copy(i, m))


    loaded("f", "r", "fg", "rg", "ex", "q", "v")
    t = lax.broadcasted_iota(jnp.int32, (rows, rows), 0)
    s = lax.broadcasted_iota(jnp.int32, (rows, rows), 1)
    lower, upper = s <= t, s >= t
    for h in range(heads):
        cols = slice(h * width, (h + 1) * width)
        q = silu(q_ref[:, cols].astype(f32))
        v = v_ref[:, cols]
        extra = jnp.broadcast_to(ex_ref[h : h + 1, :], (width, rows)).T
        scores = jnp.zeros((rows, rows), f32)
        for d, (raw_ref, gap_ref, tri) in enumerate(
            ((f_ref, fg_ref, lower), (r_ref, rg_ref, upper))
        ):
            raw = raw_ref[:, cols].astype(f32)
            key = gap_ref[:, cols] * (1.0 / (1.0 + jnp.exp(raw)))
            log = jnp.log1p(-key) + extra
            run = jnp.dot(tri.astype(f32), log, precision=highest, preferred_element_type=f32)
            last = run[rows - 1 :, :] if d == 0 else run[:1, :]
            qd = (q * jnp.exp(run)).astype(bf16)
            ki = (key * jnp.exp(-run)).astype(bf16)
            ks = (key * jnp.exp(last - run)).astype(bf16)
            scores = scores + jnp.where(tri, across(qd, ki), 0.0)
            dq[d, :, cols] = qd
            state = lax.dot_general(v, ks, (((0,), (0,)), ((), ())), preferred_element_type=f32)
            for i in range(per_head):
                st_send[h * per_head + i, d] = state[i * chunk : (i + 1) * chunk].astype(bf16)
                tot_send[h * per_head + i, d] = last
        inner[:, cols] = jnp.dot(scores.astype(bf16), v, preferred_element_type=f32)

    def plane_copy(i, j):
        src, dst = ((st_send, st_recv), (tot_send, tot_recv))[i]
        to = (p + j) % near
        return copy(src.at[to], dst.at[p], s1_s.at[i], s1_r.at[i], at(z, to))

    for j in range(1, near):
        for i in range(2):
            start(plane_copy(i, j))
    st_recv[p] = st_send[p]
    tot_recv[p] = tot_send[p]

    ring_start(u0)
    came(s1_r.at[0], st_recv.at[pl.ds(0, near - 1)])
    came(s1_r.at[1], tot_recv.at[pl.ds(0, near - 1)])

    prefix = [[None] * near, [None] * near]
    gone = [[None] * near, [None] * near]
    for d in range(2):
        state = jnp.zeros((chunk, width), f32)
        total = jnp.zeros((1, width), f32)
        for b in range(near) if d == 0 else reversed(range(near)):
            prefix[d][b], gone[d][b] = state, total
            step = tot_recv[b, d]
            state = state * jnp.exp(step) + st_recv[b, d].astype(f32)
            total = total + step
        fs_send[d] = state.astype(bf16)
        ft_send[d] = total

    def far_copy(i, d, e):
        src, dst = ((fs_send, f_recv), (ft_send, ft_recv))[i]
        to = (z + e) % far if d == 0 else (z + far - e) % far
        return copy(src.at[d], dst.at[d, e], s2_s.at[i], s2_r.at[i], at(to, p))

    def far_valid(d, e):
        return z + e < far if d == 0 else z >= e

    for e in range(1, far):
        for d in range(2):
            for i in range(2):
                start(far_copy(i, d, e), far_valid(d, e))

    ring_forward(g0)

    came(s2_r.at[0], f_recv.at[0, pl.ds(1, far - 1)])
    came(s2_r.at[1], ft_recv.at[0, pl.ds(1, far - 1)])

    for d in range(2):
        enter = jnp.zeros((chunk, width), f32)
        for e in reversed(range(1, far)):
            enter = enter * jnp.exp(ft_recv[d, e]) + f_recv[d, e].astype(f32)
        for b in range(near):
            b_send[b, d] = (enter * jnp.exp(gone[d][b]) + prefix[d][b]).astype(bf16)

    def back_copy(j):
        to = (p + j) % near
        return copy(b_send.at[to], b_recv.at[p], s3_s.at[0], s3_r.at[0], at(z, to))

    for j in range(1, near):
        start(back_copy(j))
    b_recv[p] = b_send[p]

    deal(0, 2)
    deal(1, 2)
    ring_start(g0 + 1)

    came(s3_r.at[0], b_recv.at[pl.ds(0, near - 1)])

    loaded("og", "hg")
    for h in range(heads):
        cols = slice(h * width, (h + 1) * width)
        mixed = inner[:, cols]
        for d in range(2):
            state = jnp.concatenate(
                [b_recv[h * per_head + i, d].astype(f32) for i in range(per_head)], axis=0
            ).astype(bf16)
            mixed = mixed + across(dq[d, :, cols], state)
        normed = (
            mixed
            * lax.rsqrt(jnp.mean(mixed * mixed, axis=1, keepdims=True) + head_eps)
            * hg_ref[...]
        )
        g_all[core, :, cols] = (normed * silu(og_ref[:, cols].astype(f32))).astype(bf16)

    for m in range(1, cores):
        start(copy(g_all.at[core], g_all.at[core], ga_s.at[0], ga_r.at[0], mate(m)))
    ring_forward(u0)
    ring_start(u0 + 1)
    loaded("om", "res", "ig", "ib")
    for i in range(len(pairs)):
        came(tp_r.at[i], pairs[i][1].at[pl.ds(0, cores - 1)])
    came(ga_r.at[0], g_all.at[pl.ds(0, cores - 1)])

    span = q_ref.shape[1]
    parts = []
    for b in range(cores):
        mixer = alpha_mix * res_all[b].astype(f32)
        for m in range(cores):
            mixer = mixer + jnp.dot(
                g_all[m], om_all[b, m * span : (m + 1) * span, :], preferred_element_type=f32
            )
        parts.append(mixer)
    wide = parts[0].shape[1]
    model = cores * wide
    mean = sum(jnp.sum(x, axis=1, keepdims=True) for x in parts) / model
    parts = [x - mean for x in parts]
    var = sum(jnp.sum(x * x, axis=1, keepdims=True) for x in parts) / model
    scale = lax.rsqrt(var + norm_eps)
    for b, x in enumerate(parts):
        x_all[z, b] = (x * scale * ig_all[b] + ib_all[b]).astype(bf16)

    part = rows // pieces

    def line_copy(sign, d, i, out):
        block = (z + far + ((1 if out else 0) - d) * sign) % far
        side = 0 if sign > 0 else 1
        ref = x_all.at[block, core, pl.ds(i * part, part), :]
        to = at((z + far + sign) % far, p)
        return copy(ref, ref, ag_s.at[side, d - 1, i], ag_r.at[side, d - 1, i], to)

    def line_out(sign, d):
        if sign > 0:
            return jnp.logical_and(z + 1 < far, z >= d - 1)
        return jnp.logical_and(z > 0, z + d - 1 < far)

    def line_in(sign, d):
        return z >= d if sign > 0 else z + d < far

    def line_share(sign, d, i, m):
        ref = x_all.at[(z + far - d * sign) % far, core, pl.ds(i * part, part), :]
        return copy(ref, ref, d2_s.at[0], d2_r.at[0], mate(m))

    def line_step(d, i):
        for sign in (1, -1):
            landed(line_copy(sign, d, i, False), line_in(sign, d))
            if d + 1 < far:
                start(line_copy(sign, d + 1, i, True), line_out(sign, d + 1))
            for m in range(1, cores):
                start(line_share(sign, d, i, m), line_in(sign, d))

    for i in range(pieces):
        for sign in (1, -1):
            start(line_copy(sign, 1, i, True), line_out(sign, 1))
    deal(0, 3)
    ring_start(g0 + 2)
    ring_forward(g0 + 1)
    ring_forward(u0 + 1)
    ring_start(u0 + 2)
    ring_forward(g0 + 2)
    for i in range(pieces):
        line_step(1, i)
    deal(1, 3)
    ring_start(g0 + 3)
    ring_forward(u0 + 2)
    line_step(2, 0)
    ring_forward(g0 + 3)
    for i in range(1, pieces):
        line_step(2, i)
    deal(2, 1)
    ring_start(u0 + 3)
    ring_forward(u0 + 3)
    loaded("down")
    ring_start(d0)
    for i in range(pieces):
        line_step(3, i)
    deal(2, 2)
    deal(2, 3)
    ring_start(d0 + 1)
    came(d2_r.at[0], x_all.at[pl.ds(0, far - 1), pl.ds(0, cores - 1)])
    came(half_r.at[0], wbuf.at[0, :, pl.ds(0, 2)])

    step = 256
    for n0 in range(0, units, step):
        n1 = min(units, n0 + step)
        gate = up = 0.0
        for pp in range(near):
            spots = [(zz * near + pp) * deep for zz in range(far)]
            x = jnp.concatenate(
                [
                    jnp.concatenate(
                        [x_all[j, c // wide, :, c % wide : c % wide + deep] for c in spots], axis=1
                    )
                    for j in range(far)
                ],
                axis=0,
            )
            wg, wu = (
                jnp.concatenate([wbuf[pp, zz, i, n0:n1, :] for zz in range(far)], axis=1)
                for i in range(2)
            )
            gate = gate + across(x, wg)
            up = up + across(x, wu)
        hid[:, n0:n1] = (silu(gate) * up).astype(bf16)

    close = [p] + [behind(sign, d) for d in range(1, n2) for sign in (1, -1)]
    opposite = behind(1, n2)

    def sum_copy(k, pp):
        owner = pp // share
        dst = ts_recv.at[k, pp % share, (owner + cores - 1 - core) % cores]
        return copy(ts_send.at[k, pp], dst, ts_s.at[0], ts_r.at[k, pp % share], (me, owner))

    def down(k, slots):
        w = jnp.concatenate([wbuf[pp, order[k], 2] for pp in slots], axis=1)
        y = jnp.dot(hid[...], w, preferred_element_type=f32).astype(bf16)
        for i, pp in enumerate(slots):
            ts_send[k, pp] = y[:, i * deep : (i + 1) * deep]
        for pp in slots:
            start(sum_copy(k, pp), pp // share != core)

    def reduce_copy(k, i, j):
        to = order[j + 1]
        dst = rs_recv.at[z, order[k], i]
        return copy(rs_send.at[k, i, to], dst, rs_s.at[0], rs_r.at[0], at(to, p))

    def reduce_slot(k, i):
        total = ts_send[k, core * share + i].astype(f32)
        came(ts_r.at[k, i], ts_recv.at[k, i])
        for m in range(cores - 1):
            total = total + ts_recv[k, i, m].astype(f32)
        total = total.astype(bf16)
        for j in range(far):
            rs_send[k, i, j] = total[j * rows : (j + 1) * rows]
        for j in reversed(range(far - 1)):
            start(reduce_copy(k, i, j))
        rs_recv[z, order[k], i] = rs_send[k, i, z]

    def reduce(k, late):
        for i in range(share):
            mine_late = core * share + i == opposite
            when = mine_late if late else jnp.logical_not(mine_late)
            pl.when(when)(functools.partial(reduce_slot, k, i))

    for k in range(far):
        ring_forward(d0 + k)
        down(k, close)
        if k:
            ring_done(d0 + k - 1)
            down(k - 1, [opposite])
        reduce(k, False)
        if k:
            reduce(k - 1, True)
        if k + 2 < far:
            ring_start(d0 + k + 2)
    ring_done(d0 + far - 1)
    down(far - 1, [opposite])
    reduce(far - 1, True)

    came(rs_r.at[0], rs_recv.at[pl.ds(0, far - 1)])
    mine = [
        sum(rs_recv[src, zz, i].astype(f32) for src in range(far))
        for zz in range(far)
        for i in range(share)
    ]
    fin_all[core] = jnp.concatenate(mine, axis=1).astype(bf16)

    for m in range(1, cores):
        start(copy(fin_all.at[core], fin_all.at[core], fin_s.at[0], fin_r.at[0], mate(m)))
    came(fin_r.at[0], fin_all.at[pl.ds(0, cores - 1)])
    loaded("cg", "cb")
    feed = [fin_all[c].astype(f32) for c in range(cores)]
    whole = jnp.concatenate(
        [
            feed[pp // share][:, (zz * share + pp % share) * deep : (zz * share + pp % share + 1) * deep]
            for zz in range(far)
            for pp in range(near)
        ],
        axis=1,
    )
    parts = [
        alpha_mix * x_all[z, b].astype(f32) + whole[:, b * wide : (b + 1) * wide]
        for b in range(cores)
    ]
    mean = sum(jnp.sum(x, axis=1, keepdims=True) for x in parts) / model
    parts = [x - mean for x in parts]
    var = sum(jnp.sum(x * x, axis=1, keepdims=True) for x in parts) / model
    scale = lax.rsqrt(var + norm_eps)
    for b, x in enumerate(parts):
        xs[b] = x * scale
    out_ref[...] = (xs[core] * cg_ref[...] + cb_ref[...]).astype(bf16)

    sent(deal_s.at[0], wbuf.at[0, pl.ds(0, far - 1)])
    sent(ring_s.at[0], wbuf.at[pl.ds(0, near - 1)])
    for i in range(len(pairs)):
        sent(tp_s.at[i], pairs[i][1].at[pl.ds(0, cores - 1)])
    sent(s1_s.at[0], st_recv.at[pl.ds(0, near - 1)])
    sent(s1_s.at[1], tot_recv.at[pl.ds(0, near - 1)])
    sent(s2_s.at[0], f_recv.at[0, pl.ds(1, far - 1)])
    sent(s2_s.at[1], ft_recv.at[0, pl.ds(1, far - 1)])
    sent(s3_s.at[0], b_recv.at[pl.ds(0, near - 1)])
    sent(ga_s.at[0], g_all.at[pl.ds(0, cores - 1)])
    for d in range(1, far):
        for sign in (1, -1):
            for i in range(pieces):
                pl.when(line_out(sign, d))(line_copy(sign, d, i, True).wait_send)
    sent(d2_s.at[0], x_all.at[pl.ds(0, far - 1), pl.ds(0, cores - 1)])
    sent(ts_s.at[0], ts_send.at[:, pl.ds(0, near - share)])
    sent(rs_s.at[0], rs_send.at[:, :, pl.ds(0, far - 1)])
    sent(fin_s.at[0], fin_all.at[pl.ds(0, cores - 1)])


def shards(
    query_logits, value_rows, onward_forget_logits, reverse_forget_logits, output_gate_logits,
    onward_floor_gap, reverse_floor_gap, extra_log_decay, per_head_gain, residual, output_matrix,
    inner_norm_gain, inner_norm_bias, gate_matrix, up_matrix, down_matrix,
    closing_norm_gain, closing_norm_bias,
):
    count, cores = lax.axis_size("sp"), lax.axis_size("tp")
    far = math.gcd(count, 4)
    near = count // far
    rows, span = query_logits.shape
    heads = extra_log_decay.shape[1]
    width = span // heads
    wide = residual.shape[1]
    units = gate_matrix.shape[1] // far
    deep = gate_matrix.shape[0]
    chunk = heads * width // near
    share = near // cores
    n2 = near // 2
    inner_rows = output_matrix.shape[0]
    vm = pltpu.VMEM
    dma = lambda *shape: pltpu.SemaphoreType.DMA(shape)
    scratch = [
        vm((rows, span), bf16), vm((rows, span), bf16), vm((rows, span), bf16),
        vm((rows, span), bf16), vm((rows, span), bf16), vm((1, span), f32), vm((1, span), f32),
        vm((heads, rows), f32), vm((1, width), f32), vm(gate_matrix.shape, bf16),
        vm(gate_matrix.shape, bf16), vm((1, wide), f32), vm((1, wide), f32),
        vm((near, far, 3, units, deep), bf16),
        vm((far, 2, units, deep), bf16),
        vm((near, 2, chunk, width), bf16), vm((near, 2, 1, width), f32),
        vm((near, 2, chunk, width), bf16), vm((near, 2, 1, width), f32),
        vm((2, chunk, width), bf16), vm((2, 1, width), f32),
        vm((2, far, chunk, width), bf16), vm((2, far, 1, width), f32),
        vm((near, 2, chunk, width), bf16), vm((near, 2, chunk, width), bf16),
        vm((cores, inner_rows, wide), bf16), vm((cores, rows, wide), bf16),
        vm((cores, 1, wide), f32), vm((cores, 1, wide), f32),
        vm((cores, rows, span), bf16), vm((far, cores, rows, wide), bf16),
        vm((rows, span), f32), vm((2, rows, span), bf16), vm((far * rows, units), bf16),
        vm((far, near, far * rows, deep), bf16), vm((far, share, cores - 1, far * rows, deep), bf16),
        vm((far, share, far, rows, deep), bf16), vm((far, far, share, rows, deep), bf16),
        vm((cores, rows, far * share * deep), bf16), vm((cores, rows, wide), f32),
        dma(1), dma(3, far), dma(1), dma(2, n2 - 1, 3 * far), dma(far + 1),
        dma(2), dma(2), dma(2), dma(2), dma(1), dma(1), dma(4), dma(4), dma(1), dma(1),
        dma(2, far - 1, pieces), dma(2, far - 1, pieces), dma(1), dma(1), dma(1), dma(far, share),
        dma(1), dma(1), dma(1), dma(1), dma(18),
    ]
    vmem = pl.BlockSpec(memory_space=pltpu.VMEM)
    specs = [pl.BlockSpec(memory_space=pl.ANY)] * 18
    return pl.pallas_call(
        functools.partial(layer_kernel, far, near, cores),
        out_shape=jax.ShapeDtypeStruct((rows, wide), bf16),
        in_specs=specs,
        out_specs=vmem,
        scratch_shapes=scratch,
        compiler_params=pltpu.CompilerParams(
            collective_id=0, has_side_effects=True, vmem_limit_bytes=60 * 1024 * 1024
        ),
    )(
        query_logits, value_rows, onward_forget_logits, reverse_forget_logits, output_gate_logits,
        onward_floor_gap[None], reverse_floor_gap[None], extra_log_decay.T, per_head_gain[None],
        residual, output_matrix, inner_norm_gain[None], inner_norm_bias[None], gate_matrix,
        up_matrix, down_matrix, closing_norm_gain[None], closing_norm_bias[None],
    )


def solution(mesh):
    a, b = P("sp", "tp"), P("tp")
    placed = (a, a, a, a, a, b, b, a, P(), a, P(None, "tp"), b, b, a, a, P("tp", "sp"), b, b)
    return jax.shard_map(
        shards, mesh=mesh, in_specs=placed, out_specs=P("sp", "tp"), check_vma=False
    )
```

```python
import functools
import math

import jax
import jax.numpy as jnp
from jax import lax
from jax.experimental import pallas as pl
from jax.experimental.pallas import tpu as pltpu
from jax.sharding import PartitionSpec as P

highest = lax.Precision.HIGHEST
alpha_mix = 2.0**0.25
norm_eps = 1e-05
head_eps = 1e-06
bf16 = jnp.bfloat16
f32 = jnp.float32
MESH = pl.DeviceIdType.MESH
pieces = 2


def pick(table, at):
    out = jnp.int32(table[0])
    for i, value in enumerate(table[1:], 1):
        out = jnp.where(at == i, jnp.int32(value), out)
    return out


def across(x, w):
    return lax.dot_general(x, w, (((1,), (1,)), ((), ())), preferred_element_type=f32)


def silu(x):
    return x / (1.0 + jnp.exp(-x))


def layer_kernel(
    far, near, cores,
    q_in, v_in, f_in, r_in, og_in, fg_in, rg_in, ex_in, hg_in, res_ref, om_ref, ig_ref, ib_ref,
    gate_in, up_in, down_ref, cg_in, cb_in, out_ref,
    q_ref, v_ref, f_ref, r_ref, og_ref, fg_ref, rg_ref, ex_ref, hg_ref, gate_ref, up_ref, cg_ref,
    cb_ref,
    wbuf, wsend, st_send, tot_send, st_recv, tot_recv, fs_send, ft_send, f_recv, ft_recv,
    b_send, b_recv, om_all, res_all, ig_all, ib_all, g_all, x_all, inner, dq, hid, ts_send,
    ts_recv, rs_send, rs_recv, fin_all, xs,
    deal_s, deal_r, ring_s, ring_r, half_r, s1_s, s1_r, s2_s, s2_r, s3_s, s3_r, tp_s, tp_r, ga_s, ga_r,
    ag_s, ag_r, d2_s, d2_r, ts_s, ts_r, rs_s, rs_r, fin_s, fin_r, load_s,
):
    rows = q_in.shape[0]
    heads, width = ex_in.shape[0], hg_in.shape[1]
    units, deep = wbuf.shape[3:]
    chunk = st_send.shape[2]
    per_head = near // heads
    share = near // cores
    half = (units // 2 + 15) // 16 * 16
    n2 = near // 2
    me, core = lax.axis_index("sp"), lax.axis_index("tp")
    z, p = me // near, me % near

    ring = [i ^ (i >> 1) for i in range(near)]
    spot = [ring.index(i) for i in range(near)]
    right = pick([ring[(spot[i] + 1) % near] for i in range(near)], p)
    left = pick([ring[(spot[i] - 1) % near] for i in range(near)], p)

    def behind(sign, d):
        return pick([ring[(spot[i] - sign * d) % near] for i in range(near)], p)

    partners = [sorted((j for j in range(far) if j != i), key=lambda j: (abs(j - i), j != i ^ 1))
                for i in range(far)]
    order = [z] + [pick([partners[i][k] for i in range(far)], z) for k in range(far - 1)]

    def copy(src, dst, ssem, rsem, to):
        return pltpu.make_async_remote_copy(
            src_ref=src, dst_ref=dst, send_sem=ssem, recv_sem=rsem, device_id=to,
            device_id_type=MESH,
        )

    def start(c, when=None):
        if when is None:
            c.start()
        else:
            pl.when(when)(c.start)

    def sent(sem, ref):
        copy(ref, ref, sem, sem, mate(1)).wait_send()

    def came(sem, ref):
        copy(ref, ref, sem, sem, mate(1)).wait_recv()

    def landed(c, when=None):
        if when is None:
            c.wait_recv()
        else:
            pl.when(when)(c.wait_recv)

    def at(zz, pp):
        return (zz * near + pp, core)

    def mate(m):
        return (me, (core + m) % cores)

    down_own = down_ref.at[pl.ds(pl.multiple_of(z * units, 16), units), :]
    loads = {}
    for name, src, dst in (
        ("gate", gate_in, gate_ref), ("up", up_in, up_ref), ("f", f_in, f_ref),
        ("r", r_in, r_ref), ("fg", fg_in, fg_ref), ("rg", rg_in, rg_ref), ("ex", ex_in, ex_ref),
        ("q", q_in, q_ref), ("v", v_in, v_ref), ("down", down_own, wbuf.at[p, z, 2]),
        ("om", om_ref, om_all.at[core]), ("res", res_ref, res_all.at[core]),
        ("ig", ig_ref, ig_all.at[core]), ("ib", ib_ref, ib_all.at[core]), ("og", og_in, og_ref),
        ("hg", hg_in, hg_ref), ("cg", cg_in, cg_ref), ("cb", cb_in, cb_ref),
    ):
        loads[name] = pltpu.make_async_copy(src, dst, load_s.at[len(loads)])

    def loaded(*names):
        for name in names:
            loads[name].wait()

    f_recv[...] = jnp.zeros_like(f_recv)
    ft_recv[...] = jnp.zeros_like(ft_recv)

    barrier = pltpu.get_barrier_semaphore()
    peers = [at(z, (p + j) % near) for j in range(1, near)]
    peers += [at((z + j) % far, p) for j in range(1, far)]
    peers += [mate(m) for m in range(1, cores)]
    for peer in peers:
        pl.semaphore_signal(barrier, inc=1, device_id=peer, device_id_type=MESH)

    for load in loads.values():
        load.start()
    def turn(i, ref):
        whole = ref[...].T
        for j in range(far):
            wsend[j, i] = whole[j * units : (j + 1) * units]
        wbuf[p, z, i] = wsend[z, i]

    loaded("gate")
    turn(0, gate_ref)
    pl.semaphore_wait(barrier, len(peers))

    def deal_copy(g, peer, slot, e):
        if g < 2:
            src = wsend.at[peer, g]
        else:
            src = down_ref.at[pl.ds(pl.multiple_of(peer * units, 16), units), :]
        return copy(src, wbuf.at[p, slot, g], deal_s.at[0], deal_r.at[g, slot], at(peer, p))

    def deal(g, e):
        start(deal_copy(g, (z + e) % far, z, e), z + e < far)
        start(deal_copy(g, (z + far - e) % far, z, far + e), z >= e)

    def ring_copy(k, sign, d, block):
        side = 0 if sign > 0 else 1
        ref = wbuf.at[block, order[k % far], k // far]
        if d == n2:
            ref = ref.at[pl.ds(0, half), :] if side == 0 else ref.at[pl.ds(half, units - half), :]
        to = right if sign > 0 else left
        if d < n2:
            arrive = ring_r.at[side, d - 1, k]
        else:
            arrive = half_r.at[max(0, k - 2 * far + 1)]
        return copy(ref, ref, ring_s.at[0], arrive, at(z, to))

    def ring_start(k):
        if k % far:
            landed(deal_copy(k // far, order[k % far], order[k % far], 0))
        for sign in (1, -1):
            start(ring_copy(k, sign, 1, p))

    def ring_forward(k):
        for d in range(1, n2):
            for sign in (1, -1):
                block = behind(sign, d)
                landed(ring_copy(k, sign, d, block))
                start(ring_copy(k, sign, d + 1, block))

    def ring_done(k):
        came(half_r.at[k - 2 * far + 1], wbuf.at[0, 0, 2])

    g0, u0, d0 = 0, far, 2 * far
    deal(0, 1)
    ring_start(g0)
    loaded("up")
    turn(1, up_ref)
    deal(1, 1)

    pairs = ((om_ref, om_all), (res_ref, res_all), (ig_ref, ig_all), (ib_ref, ib_all))

    def tp_copy(i, m):
        src, dst = pairs[i]
        return copy(src, dst.at[core], tp_s.at[i], tp_r.at[i], mate(m))

    for m in range(1, cores):
        for i in range(len(pairs)):
            start(tp_copy(i, m))


    loaded("f", "r", "fg", "rg", "ex", "q", "v")
    t = lax.broadcasted_iota(jnp.int32, (rows, rows), 0)
    s = lax.broadcasted_iota(jnp.int32, (rows, rows), 1)
    lower, upper = s <= t, s >= t
    for h in range(heads):
        cols = slice(h * width, (h + 1) * width)
        q = silu(q_ref[:, cols].astype(f32))
        v = v_ref[:, cols]
        extra = jnp.broadcast_to(ex_ref[h : h + 1, :], (width, rows)).T
        scores = jnp.zeros((rows, rows), f32)
        for d, (raw_ref, gap_ref, tri) in enumerate(
            ((f_ref, fg_ref, lower), (r_ref, rg_ref, upper))
        ):
            raw = raw_ref[:, cols].astype(f32)
            key = gap_ref[:, cols] * (1.0 / (1.0 + jnp.exp(raw)))
            log = jnp.log1p(-key) + extra
            run = jnp.dot(tri.astype(f32), log, precision=highest, preferred_element_type=f32)
            last = run[rows - 1 :, :] if d == 0 else run[:1, :]
            qd = (q * jnp.exp(run)).astype(bf16)
            ki = (key * jnp.exp(-run)).astype(bf16)
            ks = (key * jnp.exp(last - run)).astype(bf16)
            scores = scores + jnp.where(tri, across(qd, ki), 0.0)
            dq[d, :, cols] = qd
            state = lax.dot_general(v, ks, (((0,), (0,)), ((), ())), preferred_element_type=f32)
            for i in range(per_head):
                st_send[h * per_head + i, d] = state[i * chunk : (i + 1) * chunk].astype(bf16)
                tot_send[h * per_head + i, d] = last
        inner[:, cols] = jnp.dot(scores.astype(bf16), v, preferred_element_type=f32)

    def plane_copy(i, j):
        src, dst = ((st_send, st_recv), (tot_send, tot_recv))[i]
        to = (p + j) % near
        return copy(src.at[to], dst.at[p], s1_s.at[i], s1_r.at[i], at(z, to))

    for j in range(1, near):
        for i in range(2):
            start(plane_copy(i, j))
    st_recv[p] = st_send[p]
    tot_recv[p] = tot_send[p]

    ring_start(u0)
    came(s1_r.at[0], st_recv.at[pl.ds(0, near - 1)])
    came(s1_r.at[1], tot_recv.at[pl.ds(0, near - 1)])

    prefix = [[None] * near, [None] * near]
    gone = [[None] * near, [None] * near]
    for d in range(2):
        state = jnp.zeros((chunk, width), f32)
        total = jnp.zeros((1, width), f32)
        for b in range(near) if d == 0 else reversed(range(near)):
            prefix[d][b], gone[d][b] = state, total
            step = tot_recv[b, d]
            state = state * jnp.exp(step) + st_recv[b, d].astype(f32)
            total = total + step
        fs_send[d] = state.astype(bf16)
        ft_send[d] = total

    def far_copy(i, d, e):
        src, dst = ((fs_send, f_recv), (ft_send, ft_recv))[i]
        to = (z + e) % far if d == 0 else (z + far - e) % far
        return copy(src.at[d], dst.at[d, e], s2_s.at[i], s2_r.at[i], at(to, p))

    def far_valid(d, e):
        return z + e < far if d == 0 else z >= e

    for e in range(1, far):
        for d in range(2):
            for i in range(2):
                start(far_copy(i, d, e), far_valid(d, e))

    ring_forward(g0)

    came(s2_r.at[0], f_recv.at[0, pl.ds(1, far - 1)])
    came(s2_r.at[1], ft_recv.at[0, pl.ds(1, far - 1)])

    for d in range(2):
        enter = jnp.zeros((chunk, width), f32)
        for e in reversed(range(1, far)):
            enter = enter * jnp.exp(ft_recv[d, e]) + f_recv[d, e].astype(f32)
        for b in range(near):
            b_send[b, d] = (enter * jnp.exp(gone[d][b]) + prefix[d][b]).astype(bf16)

    def back_copy(j):
        to = (p + j) % near
        return copy(b_send.at[to], b_recv.at[p], s3_s.at[0], s3_r.at[0], at(z, to))

    for j in range(1, near):
        start(back_copy(j))
    b_recv[p] = b_send[p]

    deal(0, 2)
    deal(1, 2)
    ring_start(g0 + 1)

    came(s3_r.at[0], b_recv.at[pl.ds(0, near - 1)])

    loaded("og", "hg")
    for h in range(heads):
        cols = slice(h * width, (h + 1) * width)
        mixed = inner[:, cols]
        for d in range(2):
            state = jnp.concatenate(
                [b_recv[h * per_head + i, d].astype(f32) for i in range(per_head)], axis=0
            ).astype(bf16)
            mixed = mixed + across(dq[d, :, cols], state)
        normed = (
            mixed
            * lax.rsqrt(jnp.mean(mixed * mixed, axis=1, keepdims=True) + head_eps)
            * hg_ref[...]
        )
        g_all[core, :, cols] = (normed * silu(og_ref[:, cols].astype(f32))).astype(bf16)

    for m in range(1, cores):
        start(copy(g_all.at[core], g_all.at[core], ga_s.at[0], ga_r.at[0], mate(m)))
    ring_forward(u0)
    ring_start(u0 + 1)
    loaded("om", "res", "ig", "ib")
    for i in range(len(pairs)):
        came(tp_r.at[i], pairs[i][1].at[pl.ds(0, cores - 1)])
    came(ga_r.at[0], g_all.at[pl.ds(0, cores - 1)])

    span = q_ref.shape[1]
    parts = []
    for b in range(cores):
        mixer = alpha_mix * res_all[b].astype(f32)
        for m in range(cores):
            mixer = mixer + jnp.dot(
                g_all[m], om_all[b, m * span : (m + 1) * span, :], preferred_element_type=f32
            )
        parts.append(mixer)
    wide = parts[0].shape[1]
    model = cores * wide
    mean = sum(jnp.sum(x, axis=1, keepdims=True) for x in parts) / model
    parts = [x - mean for x in parts]
    var = sum(jnp.sum(x * x, axis=1, keepdims=True) for x in parts) / model
    scale = lax.rsqrt(var + norm_eps)
    for b, x in enumerate(parts):
        x_all[z, b] = (x * scale * ig_all[b] + ib_all[b]).astype(bf16)

    part = rows // pieces

    def line_copy(sign, d, i, out):
        block = (z + far + ((1 if out else 0) - d) * sign) % far
        side = 0 if sign > 0 else 1
        ref = x_all.at[block, core, pl.ds(i * part, part), :]
        to = at((z + far + sign) % far, p)
        return copy(ref, ref, ag_s.at[side, d - 1, i], ag_r.at[side, d - 1, i], to)

    def line_out(sign, d):
        if sign > 0:
            return jnp.logical_and(z + 1 < far, z >= d - 1)
        return jnp.logical_and(z > 0, z + d - 1 < far)

    def line_in(sign, d):
        return z >= d if sign > 0 else z + d < far

    def line_share(sign, d, i, m):
        ref = x_all.at[(z + far - d * sign) % far, core, pl.ds(i * part, part), :]
        return copy(ref, ref, d2_s.at[0], d2_r.at[0], mate(m))

    def line_step(d, i):
        for sign in (1, -1):
            landed(line_copy(sign, d, i, False), line_in(sign, d))
            if d + 1 < far:
                start(line_copy(sign, d + 1, i, True), line_out(sign, d + 1))
            for m in range(1, cores):
                start(line_share(sign, d, i, m), line_in(sign, d))

    for i in range(pieces):
        for sign in (1, -1):
            start(line_copy(sign, 1, i, True), line_out(sign, 1))
    deal(0, 3)
    ring_start(g0 + 2)
    ring_forward(g0 + 1)
    ring_forward(u0 + 1)
    ring_start(u0 + 2)
    ring_forward(g0 + 2)
    for i in range(pieces):
        line_step(1, i)
    deal(1, 3)
    ring_start(g0 + 3)
    ring_forward(u0 + 2)
    line_step(2, 0)
    ring_forward(g0 + 3)
    for i in range(1, pieces):
        line_step(2, i)
    deal(2, 1)
    ring_start(u0 + 3)
    ring_forward(u0 + 3)
    loaded("down")
    ring_start(d0)
    for i in range(pieces):
        line_step(3, i)
    deal(2, 2)
    deal(2, 3)
    ring_start(d0 + 1)
    came(d2_r.at[0], x_all.at[pl.ds(0, far - 1), pl.ds(0, cores - 1)])
    came(half_r.at[0], wbuf.at[0, :, pl.ds(0, 2)])

    step = 256
    for n0 in range(0, units, step):
        n1 = min(units, n0 + step)
        gate = up = 0.0
        for pp in range(near):
            spots = [(zz * near + pp) * deep for zz in range(far)]
            x = jnp.concatenate(
                [
                    jnp.concatenate(
                        [x_all[j, c // wide, :, c % wide : c % wide + deep] for c in spots], axis=1
                    )
                    for j in range(far)
                ],
                axis=0,
            )
            wg, wu = (
                jnp.concatenate([wbuf[pp, zz, i, n0:n1, :] for zz in range(far)], axis=1)
                for i in range(2)
            )
            gate = gate + across(x, wg)
            up = up + across(x, wu)
        hid[:, n0:n1] = (silu(gate) * up).astype(bf16)

    close = [p] + [behind(sign, d) for d in range(1, n2) for sign in (1, -1)]
    opposite = behind(1, n2)

    def sum_copy(k, pp):
        owner = pp // share
        dst = ts_recv.at[k, pp % share, (owner + cores - 1 - core) % cores]
        return copy(ts_send.at[k, pp], dst, ts_s.at[0], ts_r.at[k, pp % share], (me, owner))

    def down(k, slots):
        w = jnp.concatenate([wbuf[pp, order[k], 2] for pp in slots], axis=1)
        y = jnp.dot(hid[...], w, preferred_element_type=f32).astype(bf16)
        for i, pp in enumerate(slots):
            ts_send[k, pp] = y[:, i * deep : (i + 1) * deep]
        for pp in slots:
            start(sum_copy(k, pp), pp // share != core)

    def reduce_copy(k, i, j):
        to = order[j + 1]
        dst = rs_recv.at[z, order[k], i]
        return copy(rs_send.at[k, i, to], dst, rs_s.at[0], rs_r.at[0], at(to, p))

    def reduce_slot(k, i):
        total = ts_send[k, core * share + i].astype(f32)
        came(ts_r.at[k, i], ts_recv.at[k, i])
        for m in range(cores - 1):
            total = total + ts_recv[k, i, m].astype(f32)
        total = total.astype(bf16)
        for j in range(far):
            rs_send[k, i, j] = total[j * rows : (j + 1) * rows]
        for j in reversed(range(far - 1)):
            start(reduce_copy(k, i, j))
        rs_recv[z, order[k], i] = rs_send[k, i, z]

    def reduce(k, late):
        for i in range(share):
            mine_late = core * share + i == opposite
            when = mine_late if late else jnp.logical_not(mine_late)
            pl.when(when)(functools.partial(reduce_slot, k, i))

    for k in range(far):
        ring_forward(d0 + k)
        down(k, close)
        if k + 2 < far:
            ring_start(d0 + k + 2)
        reduce(k, False)
        if k:
            ring_done(d0 + k - 1)
            down(k - 1, [opposite])
            reduce(k - 1, True)
    ring_done(d0 + far - 1)
    down(far - 1, [opposite])
    reduce(far - 1, True)

    came(rs_r.at[0], rs_recv.at[pl.ds(0, far - 1)])
    mine = [
        sum(rs_recv[src, zz, i].astype(f32) for src in range(far))
        for zz in range(far)
        for i in range(share)
    ]
    fin_all[core] = jnp.concatenate(mine, axis=1).astype(bf16)

    for m in range(1, cores):
        start(copy(fin_all.at[core], fin_all.at[core], fin_s.at[0], fin_r.at[0], mate(m)))
    came(fin_r.at[0], fin_all.at[pl.ds(0, cores - 1)])
    loaded("cg", "cb")
    feed = [fin_all[c].astype(f32) for c in range(cores)]
    whole = jnp.concatenate(
        [
            feed[pp // share][:, (zz * share + pp % share) * deep : (zz * share + pp % share + 1) * deep]
            for zz in range(far)
            for pp in range(near)
        ],
        axis=1,
    )
    parts = [
        alpha_mix * x_all[z, b].astype(f32) + whole[:, b * wide : (b + 1) * wide]
        for b in range(cores)
    ]
    mean = sum(jnp.sum(x, axis=1, keepdims=True) for x in parts) / model
    parts = [x - mean for x in parts]
    var = sum(jnp.sum(x * x, axis=1, keepdims=True) for x in parts) / model
    scale = lax.rsqrt(var + norm_eps)
    for b, x in enumerate(parts):
        xs[b] = x * scale
    out_ref[...] = (xs[core] * cg_ref[...] + cb_ref[...]).astype(bf16)

    sent(deal_s.at[0], wbuf.at[0, pl.ds(0, far - 1)])
    sent(ring_s.at[0], wbuf.at[pl.ds(0, near - 1)])
    for i in range(len(pairs)):
        sent(tp_s.at[i], pairs[i][1].at[pl.ds(0, cores - 1)])
    sent(s1_s.at[0], st_recv.at[pl.ds(0, near - 1)])
    sent(s1_s.at[1], tot_recv.at[pl.ds(0, near - 1)])
    sent(s2_s.at[0], f_recv.at[0, pl.ds(1, far - 1)])
    sent(s2_s.at[1], ft_recv.at[0, pl.ds(1, far - 1)])
    sent(s3_s.at[0], b_recv.at[pl.ds(0, near - 1)])
    sent(ga_s.at[0], g_all.at[pl.ds(0, cores - 1)])
    for d in range(1, far):
        for sign in (1, -1):
            for i in range(pieces):
                pl.when(line_out(sign, d))(line_copy(sign, d, i, True).wait_send)
    sent(d2_s.at[0], x_all.at[pl.ds(0, far - 1), pl.ds(0, cores - 1)])
    sent(ts_s.at[0], ts_send.at[:, pl.ds(0, near - share)])
    sent(rs_s.at[0], rs_send.at[:, :, pl.ds(0, far - 1)])
    sent(fin_s.at[0], fin_all.at[pl.ds(0, cores - 1)])


def shards(
    query_logits, value_rows, onward_forget_logits, reverse_forget_logits, output_gate_logits,
    onward_floor_gap, reverse_floor_gap, extra_log_decay, per_head_gain, residual, output_matrix,
    inner_norm_gain, inner_norm_bias, gate_matrix, up_matrix, down_matrix,
    closing_norm_gain, closing_norm_bias,
):
    count, cores = lax.axis_size("sp"), lax.axis_size("tp")
    far = math.gcd(count, 4)
    near = count // far
    rows, span = query_logits.shape
    heads = extra_log_decay.shape[1]
    width = span // heads
    wide = residual.shape[1]
    units = gate_matrix.shape[1] // far
    deep = gate_matrix.shape[0]
    chunk = heads * width // near
    share = near // cores
    n2 = near // 2
    inner_rows = output_matrix.shape[0]
    vm = pltpu.VMEM
    dma = lambda *shape: pltpu.SemaphoreType.DMA(shape)
    scratch = [
        vm((rows, span), bf16), vm((rows, span), bf16), vm((rows, span), bf16),
        vm((rows, span), bf16), vm((rows, span), bf16), vm((1, span), f32), vm((1, span), f32),
        vm((heads, rows), f32), vm((1, width), f32), vm(gate_matrix.shape, bf16),
        vm(gate_matrix.shape, bf16), vm((1, wide), f32), vm((1, wide), f32),
        vm((near, far, 3, units, deep), bf16),
        vm((far, 2, units, deep), bf16),
        vm((near, 2, chunk, width), bf16), vm((near, 2, 1, width), f32),
        vm((near, 2, chunk, width), bf16), vm((near, 2, 1, width), f32),
        vm((2, chunk, width), bf16), vm((2, 1, width), f32),
        vm((2, far, chunk, width), bf16), vm((2, far, 1, width), f32),
        vm((near, 2, chunk, width), bf16), vm((near, 2, chunk, width), bf16),
        vm((cores, inner_rows, wide), bf16), vm((cores, rows, wide), bf16),
        vm((cores, 1, wide), f32), vm((cores, 1, wide), f32),
        vm((cores, rows, span), bf16), vm((far, cores, rows, wide), bf16),
        vm((rows, span), f32), vm((2, rows, span), bf16), vm((far * rows, units), bf16),
        vm((far, near, far * rows, deep), bf16), vm((far, share, cores - 1, far * rows, deep), bf16),
        vm((far, share, far, rows, deep), bf16), vm((far, far, share, rows, deep), bf16),
        vm((cores, rows, far * share * deep), bf16), vm((cores, rows, wide), f32),
        dma(1), dma(3, far), dma(1), dma(2, n2 - 1, 3 * far), dma(far + 1),
        dma(2), dma(2), dma(2), dma(2), dma(1), dma(1), dma(4), dma(4), dma(1), dma(1),
        dma(2, far - 1, pieces), dma(2, far - 1, pieces), dma(1), dma(1), dma(1), dma(far, share),
        dma(1), dma(1), dma(1), dma(1), dma(18),
    ]
    vmem = pl.BlockSpec(memory_space=pltpu.VMEM)
    specs = [pl.BlockSpec(memory_space=pl.ANY)] * 18
    return pl.pallas_call(
        functools.partial(layer_kernel, far, near, cores),
        out_shape=jax.ShapeDtypeStruct((rows, wide), bf16),
        in_specs=specs,
        out_specs=vmem,
        scratch_shapes=scratch,
        compiler_params=pltpu.CompilerParams(
            collective_id=0, has_side_effects=True, vmem_limit_bytes=60 * 1024 * 1024
        ),
    )(
        query_logits, value_rows, onward_forget_logits, reverse_forget_logits, output_gate_logits,
        onward_floor_gap[None], reverse_floor_gap[None], extra_log_decay.T, per_head_gain[None],
        residual, output_matrix, inner_norm_gain[None], inner_norm_bias[None], gate_matrix,
        up_matrix, down_matrix, closing_norm_gain[None], closing_norm_bias[None],
    )


def solution(mesh):
    a, b = P("sp", "tp"), P("tp")
    placed = (a, a, a, a, a, b, b, a, P(), a, P(None, "tp"), b, b, a, a, P("tp", "sp"), b, b)
    return jax.shard_map(
        shards, mesh=mesh, in_specs=placed, out_specs=P("sp", "tp"), check_vma=False
    )
```
